256 devices in a mesh: sp: 64 (over z, x, core), tp: 4 (over y).
Axes of the slice: x: 4, y: 4, z: 8, core: 2. Of those that a mesh axis runs over, the one named last changes fastest.
Arguments:
- result_cotangent_values: bfloat16 [8192, 2048], P('sp'), may hold values from -16 to 16
- specialist_entry_vectors: bfloat16 [8192, 2048], P('sp'), may hold values from -6 to 6
- chosen_specialists: int32 [8192, 2], P('sp'), may hold values from 0 to 31, all different within a row; in each aligned block of 128 rows (0 to 127, 128 to 255, ...) at most 16 rows name the same one
- specialist_mixing_shares: float32 [8192, 2], P('sp'), may hold values from 0.1 to 0.9
- specialist_switch_maps: bfloat16 [64, 2048, 1792], P('sp', None, 'tp'), may hold values from -0.125 to 0.125
- specialist_widen_maps: bfloat16 [64, 2048, 1792], P('sp', None, 'tp'), may hold values from -0.125 to 0.125
- specialist_shrink_maps: bfloat16 [64, 1792, 2048], P('sp', 'tp'), may hold values from -0.09375 to 0.09375
- memory_readout_map: bfloat16 [2048, 2048], P('sp', 'tp'), may hold values from -0.125 to 0.125
- memory_source_vectors: bfloat16 [8192, 2048], P('sp', 'tp'), may hold values from -6 to 6
- memory_hidden_values: bfloat16 [8192, 2048], P('sp', 'tp'), may hold values from -6 to 6
- feature_fading_speed: float32 [2048], P('tp'), may hold values from 2.03450521e-06 to 0.009
- extra_log_fading: float32 [8192], P('sp'), may hold values from -2.8 to 0
- memory_switch_tiles: bfloat16 [8, 256, 256], P('tp'), may hold values from -0.375 to 0.375
- entry_switch_tiles: bfloat16 [8, 256, 256], P('tp'), may hold values from -0.375 to 0.375
Outputs:
- gate_proj_grad: bfloat16 [64, 2048, 1792], P('sp', None, 'tp')
- up_proj_grad: bfloat16 [64, 2048, 1792], P('sp', None, 'tp')
- down_proj_grad: bfloat16 [64, 1792, 2048], P('sp', 'tp')
- out_proj_grad: float32 [2048, 2048], P('sp', 'tp')
- lru_input_grad: float32 [8192, 2048], P('sp', 'tp')
The draws below stay inside these ranges and needn't reach their ends.
Inputs may be any that keep to these rules, and one draw needn't show every extreme that they name: `chosen_specialists`: each token names two different experts; among the 128 tokens of one device no expert is named more than 16 times, a bound that some block reaches on some device.
All inputs are finite; a program needn't handle non-finite values.
Results may differ from the reference program's by a relative error of at most 0.009.
Values may be sent and summed in bfloat16 or wider, within the bound.
A program may use at most 128 MiB of HBM per device.

```python
import math
import jax
import jax.numpy as jnp
import numpy as np
from jax import lax

D = 2048
FE = 3584
BLOCKS = 8
SLICES = 2
TOPK = 2
TOK_DEV = 128
SEQ = 8192
BW = 256
EXPERTS = 32
CAPACITY = 16
FE_PART = 1792
PARTS_SIZE = 8
FE_DEV = 448
N_SP = 64
N_TP = 4


def draw_feature_fading_speed(key, part):
    pick_key, slow_key, fast_key = jax.random.split(key, 3)
    share = 0.5
    slow_mask = jax.random.uniform(pick_key, (D,), jnp.float32) < share
    slow_rate = jnp.exp(jax.random.uniform(slow_key, (D,), jnp.float32, jnp.log(0.02), jnp.log(0.25))) / SEQ
    fast_rate = jnp.exp(jax.random.uniform(fast_key, (D,), jnp.float32, jnp.log(0.005), jnp.log(0.0085)))
    return jnp.where(slow_mask, slow_rate, fast_rate)


def draw_extra_log_fading(key, part):
    where_key, size_key = jax.random.split(key)
    spots = jax.random.randint(where_key, (4,), 0, SEQ)
    keeping = jax.random.uniform(size_key, (4,), jnp.float32, 0.5, 0.8)
    hits = (jnp.arange(SEQ, dtype=jnp.int32)[:, None] == spots[None, :]).astype(jnp.float32)
    return jnp.sum(hits * jnp.log(keeping)[None, :], axis=1)


def spiked(values, key, source, target, shards_of, factor):
    def block_of(dim):
        return (jnp.arange(values.shape[dim]) // (values.shape[dim] // shards_of)).reshape((-1,) + (1,) * (values.ndim - 1 - dim))

    one_side = jax.random.permutation(key, shards_of)[block_of(target)]
    second = (block_of(target) + shards_of // 2) % shards_of
    return jnp.where((block_of(source) == one_side) | (block_of(source) == second), factor * values, values)


def level_of(stream_key, shape, cuts, low, top_value):
    def one(position, shards_of):
        heights = jax.random.uniform(jax.random.fold_in(jax.random.fold_in(stream_key, 6), position), (shards_of,), jnp.float32, low / len(cuts), top_value / len(cuts))
        return jnp.repeat(jnp.exp(heights), shape[position] // shards_of).reshape((-1,) + (1,) * (len(shape) - position - 1))

    factor_of = one(*cuts[0])
    for cut in cuts[1:]:
        factor_of = factor_of * one(*cut)
    return factor_of


def shared_out(rng, own, number, rows, count, top, reach, lean):
    order = jax.random.permutation(rng, count)
    heavy_load, ordinary = portions_of(count, rows * top, reach, lean, True), portions_of(count, rows * top, reach, lean, False)
    places = jnp.arange(count)

    def named(tallies, offset_by):
        used = int((tallies > 0).sum())
        fixed = max(1, used // 4)
        passed = fixed + (places - fixed + offset_by * (used - fixed)) % max(1, count - fixed)
        return jnp.zeros((count,), jnp.int32).at[order[jnp.where(places < fixed, places, passed)]].set(jnp.asarray(tallies, jnp.int32))

    tallies = jnp.where(number % 4 == 0, named(heavy_load, number // 4), named(ordinary, number - number // 4 - 1))
    mixed = jax.random.permutation(jax.random.fold_in(own, 3), count)
    donor, receiver = mixed[0:count // 2 * 2:2], mixed[1:count // 2 * 2:2]
    room = jnp.minimum(tallies[donor] - 1, reach - tallies[receiver]) // 2
    room = jnp.where((donor == order[0]) | (receiver == order[0]) | (tallies[receiver] == 0), 0, jnp.maximum(room, 0))
    passed = jax.random.randint(jax.random.fold_in(own, 4), (count // 2,), 0, 1 << 20) % (room + 1)
    tallies = tallies.at[donor].add(-passed).at[receiver].add(passed)
    items = jnp.searchsorted(jnp.cumsum(tallies), jnp.arange(rows * top), side="right").astype(jnp.int32)
    listing = items.reshape(top, rows).T
    listing = listing[jax.random.permutation(jax.random.fold_in(own, 1), rows)]
    offset_by = jax.random.randint(jax.random.fold_in(own, 2), (rows, 1), 0, top)
    return jnp.take_along_axis(listing, (jnp.arange(top)[None, :] + offset_by) % top, axis=1)


def portions_of(count, total, most, slope, full):
    weights = [(1 << 20) // math.isqrt(rank ** slope) + 1 for rank in range(1, count + 1)]
    largest = most if full else min(most, max(-(-total // count), total * weights[0] // sum(weights)))
    least = 1 if total - largest >= count - 1 else 0
    given, spare = [largest] + [least] * (count - 1), total - largest - least * (count - 1)
    while spare > 0:
        free = [i for i in range(1, count) if given[i] < largest] or [i for i in range(1, count) if given[i] < most]
        pool, remaining = sum([weights[i] for i in free]), spare
        for i in free:
            more = min(most - given[i], max(1, remaining * weights[i] // pool), spare)
            given[i] = given[i] + more
            spare = spare - more
    return np.array(given)


def scatter_about(key, dims, width, limit, pieces=(), held_as=jnp.bfloat16):
    result = jax.random.normal(key, dims, jnp.float32) * width
    if len(pieces) > 0:
        result = level_of(key, dims, pieces, -0.22, 0.18) * result
    return jnp.clip(result, min=-limit, max=limit).astype(held_as)


def bell_draw_with(key, extent, deviation, bound, shards, heavy, held_as=jnp.bfloat16):
    entries = deviation * jax.random.normal(key, extent, jnp.float32)
    if shards:
        entries = entries * level_of(key, extent, shards, -0.22, 0.18)
    return jnp.clip(spiked(entries, jax.random.fold_in(key, 3), *heavy), -bound, bound).astype(held_as)


def setup_inputs(seed: int = 0) -> dict:
    keys = jax.random.split(jax.random.key(seed), 15)
    result_cotangent_values = bell_draw_with(keys[0], (SEQ, D), 1.0, 16.0, ((0, 64),), (0, 1, 64, 4.0))
    specialist_entry_vectors = scatter_about(keys[1], (SEQ, D), 1.0, 6.0, ((0, 64),))
    chosen_specialists_keys = jax.random.split(jax.random.fold_in(keys[2], 1), SEQ // TOK_DEV)
    chosen_specialists_turns = jax.random.permutation(jax.random.fold_in(keys[2], 3), SEQ // TOK_DEV)
    chosen_specialists = jax.vmap(lambda own, number: shared_out(jax.random.fold_in(keys[2], 2), own, number, TOK_DEV, EXPERTS, TOPK, CAPACITY, 1))(chosen_specialists_keys, chosen_specialists_turns).reshape((SEQ, TOPK))
    specialist_mixing_shares = jnp.clip(0.1 + 0.79999997 * jax.random.uniform(keys[3], (SEQ, TOPK), jnp.float32) ** level_of(keys[3], (SEQ, TOPK), ((0, 64),), -0.2, 0.2), 0.1, 0.9)
    specialist_switch_maps = scatter_about(keys[4], (EXPERTS * SLICES, D, FE_PART), D ** -0.5, 0.125, ((0, 64), (2, 4)))
    specialist_widen_maps = scatter_about(keys[5], (EXPERTS * SLICES, D, FE_PART), D ** -0.5, 0.125, ((0, 64), (2, 4)))
    specialist_shrink_maps = scatter_about(keys[6], (EXPERTS * SLICES, FE_PART, D), FE ** -0.5, 0.09375, ((0, 64), (1, 4)))
    memory_readout_map = scatter_about(keys[7], (D, D), D ** -0.5, 0.125, ((0, 64), (1, 4)))
    memory_source_vectors = scatter_about(keys[8], (SEQ, D), 1.0, 6.0, ((0, 64), (1, 4)))
    memory_hidden_values = scatter_about(keys[9], (SEQ, D), 1.0, 6.0, ((0, 64), (1, 4)))
    feature_fading_speed = draw_feature_fading_speed(jax.random.fold_in(keys[14], 71), 0)
    extra_log_fading = draw_extra_log_fading(jax.random.fold_in(keys[14], 71), 0)
    memory_switch_tiles = scatter_about(keys[12], (BLOCKS, BW, BW), BW ** -0.5, 0.375, ((0, 4),))
    entry_switch_tiles = scatter_about(keys[13], (BLOCKS, BW, BW), BW ** -0.5, 0.375, ((0, 4),))
    return dict(result_cotangent_values=result_cotangent_values, specialist_entry_vectors=specialist_entry_vectors, chosen_specialists=chosen_specialists, specialist_mixing_shares=specialist_mixing_shares, specialist_switch_maps=specialist_switch_maps, specialist_widen_maps=specialist_widen_maps, specialist_shrink_maps=specialist_shrink_maps, memory_readout_map=memory_readout_map, memory_source_vectors=memory_source_vectors, memory_hidden_values=memory_hidden_values, feature_fading_speed=feature_fading_speed, extra_log_fading=extra_log_fading, memory_switch_tiles=memory_switch_tiles, entry_switch_tiles=entry_switch_tiles)


def silu_slope(value):
    sig_value = jax.nn.sigmoid(value)
    return sig_value * (1.0 + value * (1.0 - sig_value))

def compose(upper_map, lower_map):
    return (lower_map[0] * upper_map[0], lower_map[1] + lower_map[0] * upper_map[1])

def slot_index(chosen_specialists):
    flat_expert = chosen_specialists.reshape(N_SP, TOPK * TOK_DEV)
    onehot = (flat_expert[:, :, None] == jnp.arange(EXPERTS, dtype=jnp.int32)[None, None, :]).astype(jnp.int32)
    slot_rank = lax.optimization_barrier(jnp.sum((jnp.cumsum(onehot, axis=1) - 1) * onehot, axis=2))
    source = jnp.arange(N_SP, dtype=jnp.int32)[:, None]
    index = (flat_expert * N_SP + source) * CAPACITY + slot_rank
    return index.reshape(-1).astype(jnp.int32)

def expert_pass(args):
    inputs, grads_in, gate_weight, up_weight, down_weight = args
    x_val = inputs.astype(jnp.float32)
    y_val = grads_in.astype(jnp.float32)
    gate_full = gate_weight.astype(jnp.float32)
    up_full = up_weight.astype(jnp.float32)
    down_full = down_weight.astype(jnp.float32)
    gate_value = jnp.einsum('rd,pdf->prf', x_val, gate_full)
    up_value = jnp.einsum('rd,pdf->prf', x_val, up_full)
    active = jax.nn.silu(gate_value)
    hidden = lax.optimization_barrier((active * up_value).astype(jnp.bfloat16)).astype(jnp.float32)
    down_grad = jnp.einsum('prf,rd->pfd', hidden, y_val).astype(jnp.bfloat16)
    hidden_grad = jnp.einsum('rd,pfd->prf', y_val, down_full)
    gate_grad = lax.optimization_barrier((hidden_grad * up_value * silu_slope(gate_value)).astype(jnp.bfloat16)).astype(jnp.float32)
    up_grad = lax.optimization_barrier((hidden_grad * active).astype(jnp.bfloat16)).astype(jnp.float32)
    gate_weight_grad = jnp.einsum('rd,prf->pdf', x_val, gate_grad).astype(jnp.bfloat16)
    up_weight_grad = jnp.einsum('rd,prf->pdf', x_val, up_grad).astype(jnp.bfloat16)
    token_part = jnp.einsum('prf,pdf->prd', gate_grad, gate_full) + jnp.einsum('prf,pdf->prd', up_grad, up_full)
    rounded = lax.optimization_barrier(token_part.astype(jnp.bfloat16)).astype(jnp.float32)
    return (gate_weight_grad, up_weight_grad, down_grad, lax.optimization_barrier(jnp.sum(rounded, axis=0)))

def reference(result_cotangent_values, specialist_entry_vectors, chosen_specialists, specialist_mixing_shares, specialist_switch_maps, specialist_widen_maps, specialist_shrink_maps, memory_readout_map, memory_source_vectors, memory_hidden_values, feature_fading_speed, extra_log_fading, memory_switch_tiles, entry_switch_tiles):
    index = slot_index(chosen_specialists)
    sent = (specialist_mixing_shares[:, :, None] * result_cotangent_values[:, None, :].astype(jnp.float32)).astype(jnp.bfloat16).reshape(SEQ * TOPK, D)
    copies = jnp.broadcast_to(specialist_entry_vectors[:, None, :], (SEQ, TOPK, D)).reshape(SEQ * TOPK, D)
    total_rows = EXPERTS * N_SP * CAPACITY
    grads_in = jnp.zeros((total_rows, D), jnp.bfloat16).at[index].set(sent).reshape(EXPERTS, N_SP * CAPACITY, D)
    inputs = jnp.zeros((total_rows, D), jnp.bfloat16).at[index].set(copies).reshape(EXPERTS, N_SP * CAPACITY, D)
    gate_parts = specialist_switch_maps.reshape(EXPERTS, SLICES, D, N_TP, FE_DEV).transpose(0, 1, 3, 2, 4).reshape(EXPERTS, PARTS_SIZE, D, FE_DEV)
    up_parts = specialist_widen_maps.reshape(EXPERTS, SLICES, D, N_TP, FE_DEV).transpose(0, 1, 3, 2, 4).reshape(EXPERTS, PARTS_SIZE, D, FE_DEV)
    down_parts = specialist_shrink_maps.reshape(EXPERTS, PARTS_SIZE, FE_DEV, D)
    gate_grads, up_grads, down_grads, partials = lax.map(expert_pass, (inputs, grads_in, gate_parts, up_parts, down_parts))
    moe_grad = jnp.take(partials.reshape(total_rows, D), index, axis=0).reshape(SEQ, TOPK, D).sum(axis=1)
    mixed_grad = (result_cotangent_values.astype(jnp.float32) + moe_grad).astype(jnp.bfloat16)
    upstream = jnp.dot(mixed_grad, memory_readout_map, preferred_element_type=jnp.float32)
    xin = memory_source_vectors.astype(jnp.float32)
    blocks_in = xin.reshape(SEQ, BLOCKS, BW)
    rec_full = memory_switch_tiles.astype(jnp.float32)
    in_full = entry_switch_tiles.astype(jnp.float32)
    memory_switch_fraction = jax.nn.sigmoid(jnp.einsum('tnc,ncd->tnd', blocks_in, rec_full).reshape(SEQ, D))
    inp_open = jax.nn.sigmoid(jnp.einsum('tnc,ncd->tnd', blocks_in, in_full).reshape(SEQ, D))
    log_fading_factor = -8.0 * memory_switch_fraction * feature_fading_speed[None, :] + extra_log_fading[:, None]
    decay_mult = jnp.exp(log_fading_factor)
    spare_room = -jnp.expm1(2.0 * log_fading_factor)
    in_scale = jnp.sqrt(jnp.maximum(spare_room, 0.01))
    drive = in_scale * inp_open * xin
    coeff = jnp.concatenate([decay_mult[1:], jnp.ones((1, D), jnp.float32)], axis=0)
    _, dstate = lax.associative_scan(compose, (coeff, upstream), reverse=True, axis=0)
    scale_slope = jnp.where(spare_room > 0.01, -decay_mult * decay_mult / in_scale, 0.0)
    log_grad = dstate * (memory_hidden_values.astype(jnp.float32) - drive + scale_slope * inp_open * xin)
    grad_rec = lax.optimization_barrier((log_grad * (-8.0 * feature_fading_speed[None, :]) * memory_switch_fraction * (1.0 - memory_switch_fraction)).astype(jnp.bfloat16)).astype(jnp.float32)
    grad_in = lax.optimization_barrier((dstate * in_scale * xin * inp_open * (1.0 - inp_open)).astype(jnp.bfloat16)).astype(jnp.float32)
    back_rec = jnp.einsum('tnd,ncd->tnc', grad_rec.reshape(SEQ, BLOCKS, BW), rec_full).reshape(SEQ, D)
    back_in = jnp.einsum('tnd,ncd->tnc', grad_in.reshape(SEQ, BLOCKS, BW), in_full).reshape(SEQ, D)
    lru_input_grad = dstate * in_scale * inp_open + back_rec + back_in
    out_proj_grad = jnp.dot(mixed_grad.T, memory_hidden_values, preferred_element_type=jnp.float32)
    gate_proj_grad = gate_grads.reshape(EXPERTS, SLICES, N_TP, D, FE_DEV).transpose(0, 1, 3, 2, 4).reshape(EXPERTS * SLICES, D, N_TP * FE_DEV)
    up_proj_grad = up_grads.reshape(EXPERTS, SLICES, N_TP, D, FE_DEV).transpose(0, 1, 3, 2, 4).reshape(EXPERTS * SLICES, D, N_TP * FE_DEV)
    down_proj_grad = down_grads.reshape(EXPERTS * SLICES, N_TP * FE_DEV, D)
    return (gate_proj_grad, up_proj_grad, down_proj_grad, out_proj_grad, lru_input_grad)
```

```python
import functools

import jax
import jax.numpy as jnp
from jax import lax
from jax.experimental import pallas as pl
from jax.experimental.pallas import tpu as pltpu
from jax.sharding import Mesh
from jax.sharding import PartitionSpec as P

SLICES = 2
SP = ("sp_0", "sp_1", "sp_2")
MESH = pl.DeviceIdType.MESH
F32, BF16 = jnp.float32, jnp.bfloat16


def place():
    return tuple(lax.axis_index(n) for n in ("sp_0", "sp_1", "sp_2", "tp"))


def offset_of(k, count):
    odd = lax.rem(k, 2)
    return lax.rem(odd * ((k + 1) // 2) + (1 - odd) * (count - k // 2), count)


def greet_peers(dims, far_share):
    nz, nx, ny = dims
    z, x, c, y = place()
    barrier = pltpu.get_barrier_semaphore()

    def greet(i, _):
        to = (lax.rem(z + i // nx, nz), lax.rem(x + lax.rem(i, nx), nx), c, y)
        pl.semaphore_signal(barrier, inc=1, device_id=to, device_id_type=MESH)
        return 0

    lax.fori_loop(1, nz * nx, greet, 0)
    steps = (1, 2, 3) if far_share else (1, 3)
    for step in steps:
        to = (z, x, c, lax.rem(y + step, ny))
        pl.semaphore_signal(barrier, inc=1, device_id=to, device_id_type=MESH)
    pl.semaphore_signal(barrier, inc=1, device_id=(z, x, 1 - c, y), device_id_type=MESH)
    return barrier, nz * nx - 1 + len(steps) + 1


def drained(ref, sem):
    pltpu.make_async_copy(ref, ref, sem).wait()


def dispatch_kernel(
    dims, cap, target, share, cot, rows, out, slots, own_sem, d_send, d_recv, y_send, y_recv,
    f_send, f_recv, c_send, c_recv,
):
    nz, nx, ny = dims
    z, x, c, y = place()
    barrier, greetings = greet_peers(dims, False)
    width = cot.shape[1] // ny
    half = nz * nx * cap
    group = nx * cap
    cols = pl.ds(pl.multiple_of(y * width, 128), width)

    slot = lax.broadcasted_iota(jnp.int32, (half, target.shape[1]), 0)
    onehot = jnp.where(slot == target[...], 1.0, 0.0).astype(BF16)
    some = rows[:, cols]
    slots[0] = jnp.dot(
        onehot, jnp.concatenate([some, some], axis=0), preferred_element_type=F32
    ).astype(BF16)
    some = cot[:, cols].astype(F32)
    scaled = [(share[:, k : k + 1] * some).astype(BF16) for k in range(2)]
    slots[1] = jnp.dot(
        onehot, jnp.concatenate(scaled, axis=0), preferred_element_type=F32
    ).astype(BF16)

    pl.semaphore_wait(barrier, greetings)

    def source(e):
        return slots.at[:, pl.ds(pl.multiple_of(e * cap, cap), cap), :]

    def target_rows(k):
        start = pl.multiple_of(c * half + (k * nx + x) * cap, cap)
        return out.at[:, pl.ds(start, cap), cols]

    own = pltpu.make_async_copy(source(z * nx + x), target_rows(0), own_sem)
    own.start()

    def push(i, _):
        k, dx = i // nx, lax.rem(i, nx)
        tz, tx = lax.rem(z + offset_of(k, nz), nz), lax.rem(x + dx, nx)
        pltpu.make_async_remote_copy(
            src_ref=source(tz * nx + tx),
            dst_ref=target_rows(k),
            send_sem=d_send,
            recv_sem=d_recv.at[k],
            device_id=(tz, tx, c, y),
            device_id_type=MESH,
        ).start()
        return 0

    lax.fori_loop(1, nz * nx, push, 0)

    def block(k, turn):
        start = pl.multiple_of(c * half + k * group, cap)
        share_of = lax.rem(y + turn, ny)
        return out.at[
            :, pl.ds(start, group), pl.ds(pl.multiple_of(share_of * width, 128), width)
        ]

    def across(k, turn):
        pltpu.make_async_remote_copy(
            src_ref=block(k, turn),
            dst_ref=block(k, turn),
            send_sem=c_send,
            recv_sem=c_recv,
            device_id=(z, x, 1 - c, y),
            device_id_type=MESH,
        ).start()

    def along(k, turn, step, send, recv):
        copy = pltpu.make_async_remote_copy(
            src_ref=block(k, turn),
            dst_ref=block(k, turn),
            send_sem=send,
            recv_sem=recv,
            device_id=(z, x, c, lax.rem(y + step, ny)),
            device_id_type=MESH,
        )
        copy.start()

    for turn in range(nz + 3):
        k = turn
        if k < nz:
            if k == 0:
                drained(slots.at[:, pl.ds(0, group - cap), :], d_recv.at[0])
                own.wait()
            else:
                drained(block(k, 0), d_recv.at[k])
            along(k, 0, 1, y_send.at[0, k], y_recv.at[0, k])
            along(k, 0, 3, y_send.at[1, k], y_recv.at[1, k])
            across(k, 0)
        k = turn - 2
        if 0 <= k < nz:
            drained(block(k, 3), y_recv.at[0, k])
            if k % 2 == 0:
                along(k, 3, 1, f_send.at[k], f_recv.at[k])
            across(k, 3)
            drained(block(k, 1), y_recv.at[1, k])
            if k % 2 == 1:
                along(k, 1, 3, f_send.at[k], f_recv.at[k])
            across(k, 1)
        k = turn - 3
        if 0 <= k < nz:
            drained(block(k, 2), f_recv.at[k])
            across(k, 2)

    whole = out.at[:, pl.ds(pl.multiple_of((1 - c) * half, cap), half), :]
    drained(whole, c_recv)
    drained(whole, c_send)
    drained(slots.at[:, pl.ds(0, half - cap), :], d_send)
    for k in range(nz):
        drained(block(k, 0), y_send.at[0, k])
        drained(block(k, 0), y_send.at[1, k])
        drained(block(k, 2), f_send.at[k])


def dispatched(dims, cap, target, share, cot, rows):
    nz, nx, ny = dims
    half = nz * nx * cap
    vmem = pl.BlockSpec(memory_space=pltpu.VMEM)
    dma = pltpu.SemaphoreType.DMA
    return pl.pallas_call(
        functools.partial(dispatch_kernel, dims, cap),
        out_shape=jax.ShapeDtypeStruct((2, 2 * half, cot.shape[1]), BF16),
        in_specs=[vmem] * 4,
        out_specs=pl.BlockSpec(memory_space=pl.ANY),
        scratch_shapes=[
            pltpu.VMEM((2, half, cot.shape[1] // ny), BF16),
            dma, dma, dma((nz,)), dma((2, nz)), dma((2, nz)), dma((nz,)), dma((nz,)), dma, dma,
        ],
        compiler_params=pltpu.CompilerParams(collective_id=0, has_side_effects=True),
        name="dispatch",
    )(target, share, cot, rows)


def return_kernel(
    dims, cap, part, target, cot, out, pair, sums, far, near, back, mine, moe, own_sem,
    p_send, p_recv, y_send, y_recv, r_send, r_recv, m_send, m_recv,
):
    nz, nx, ny = dims
    z, x, c, y = place()
    barrier, greetings = greet_peers(dims, True)
    width = cot.shape[1] // ny
    half = nz * nx * cap
    mid = half // 2
    pl.semaphore_wait(barrier, greetings)

    def cols(turn):
        return pl.ds(pl.multiple_of(lax.rem(y + turn, ny) * width, 128), width)

    def remote(src, dst, send, recv, to):
        pltpu.make_async_remote_copy(
            src_ref=src, dst_ref=dst, send_sem=send, recv_sem=recv, device_id=to,
            device_id_type=MESH,
        ).start()

    theirs = pl.ds(pl.multiple_of((1 - c) * half, cap), half)
    ours = pl.multiple_of(c * half, cap)
    order = (2, 1, 3, 0)
    for turn in order:
        remote(
            part.at[theirs, cols(turn)], pair.at[turn], p_send.at[turn], p_recv.at[turn],
            (z, x, 1 - c, y),
        )
    up, down = (z, x, c, lax.rem(y + 1, ny)), (z, x, c, lax.rem(y + 3, ny))
    low, high = pl.ds(0, mid), pl.ds(mid, mid)

    def added(turn):
        drained(pair.at[turn], p_recv.at[turn])

        def some(i, _):
            here = pl.multiple_of(i * 64, 64)
            total = part[pl.ds(ours + here, 64), cols(turn)].astype(F32)
            total = total + pair[turn, pl.ds(here, 64), :].astype(F32)
            sums[turn, pl.ds(here, 64), :] = total.astype(BF16)
            return 0

        lax.fori_loop(0, half // 64, some, 0)

    added(2)
    remote(sums.at[2, low], far.at[0], y_send.at[0], y_recv.at[0], up)
    remote(sums.at[2, high], far.at[1], y_send.at[1], y_recv.at[1], down)
    added(1)
    remote(sums.at[1, high], near.at[0, high], y_send.at[2], y_recv.at[2], up)
    added(3)
    remote(sums.at[3, low], near.at[1, low], y_send.at[3], y_recv.at[3], down)
    added(0)

    def joined(side, turn, first):
        drained(far.at[side], y_recv.at[side])

        def some(i, _):
            here = pl.multiple_of(i * 64, 64)
            total = sums[turn, pl.ds(first + here, 64), :].astype(F32)
            total = total + far[side, pl.ds(here, 64), :].astype(F32)
            sums[turn, pl.ds(first + here, 64), :] = total.astype(BF16)
            return 0

        lax.fori_loop(0, mid // 64, some, 0)

    joined(0, 1, 0)
    remote(sums.at[1, low], near.at[0, low], y_send.at[4], y_recv.at[4], up)
    joined(1, 3, mid)
    remote(sums.at[3, high], near.at[1, high], y_send.at[5], y_recv.at[5], down)

    me = z * nx + x

    def finished(first, early, late):
        drained(far.at[0], y_recv.at[early])
        drained(far.at[0], y_recv.at[late])

        def some(i, _):
            here = pl.multiple_of(first + i * 64, 64)
            total = sums[0, pl.ds(here, 64), :].astype(F32)
            total = total + near[0, pl.ds(here, 64), :].astype(F32)
            total = total + near[1, pl.ds(here, 64), :].astype(F32)
            mine[pl.ds(here, 64), :] = total.astype(BF16)
            return 0

        lax.fori_loop(0, mid // 64, some, 0)

    def give(i, _):
        k, sx = i // nx, lax.rem(i, nx)
        sx = lax.rem(x + sx, nx)
        to = (lax.rem(z + nz - offset_of(k, nz), nz), sx, c, y)
        remote(
            mine.at[pl.ds(pl.multiple_of((k * nx + sx) * cap, cap), cap), :],
            back.at[pl.ds(pl.multiple_of(me * cap, cap), cap), :],
            r_send, r_recv, to,
        )
        return 0

    finished(mid, 2, 5)
    lax.fori_loop(nz * nx // 2, nz * nx, give, 0)
    finished(0, 4, 3)
    own = pltpu.make_async_copy(
        mine.at[pl.ds(pl.multiple_of(x * cap, cap), cap), :],
        back.at[pl.ds(pl.multiple_of(me * cap, cap), cap), :],
        own_sem,
    )
    own.start()
    lax.fori_loop(1, nz * nx // 2, give, 0)
    slot = lax.broadcasted_iota(jnp.int32, (cot.shape[0], half), 1)
    chosen = (slot == target[:, 0:1]) | (slot == target[:, 1:2])
    onehot = jnp.where(chosen, 1.0, 0.0).astype(BF16)
    own.wait()
    drained(back.at[pl.ds(0, half - cap), :], r_recv)
    moe[:, cols(0)] = jnp.dot(onehot, back[...], preferred_element_type=F32).astype(BF16)
    for step in (1, 3, 2):
        remote(
            moe.at[:, cols(0)], moe.at[:, cols(0)], m_send.at[step - 1], m_recv.at[step - 1],
            (z, x, c, lax.rem(y + step, ny)),
        )
    for step in (1, 3, 2):
        drained(moe.at[:, cols(ny - step)], m_recv.at[step - 1])
    out[...] = (cot[...].astype(F32) + moe[...].astype(F32)).astype(BF16)

    for turn in range(4):
        drained(pair.at[turn], p_send.at[turn])
    for i in range(6):
        drained(far.at[0], y_send.at[i])
    drained(back.at[pl.ds(0, half - cap), :], r_send)
    for step in (1, 2, 3):
        drained(moe.at[:, cols(0)], m_send.at[step - 1])


def returned(dims, cap, part, target, cot):
    nz, nx, ny = dims
    half, width = nz * nx * cap, cot.shape[1] // ny
    vmem = pl.BlockSpec(memory_space=pltpu.VMEM)
    dma = pltpu.SemaphoreType.DMA
    return pl.pallas_call(
        functools.partial(return_kernel, dims, cap),
        out_shape=jax.ShapeDtypeStruct(cot.shape, BF16),
        in_specs=[vmem] * 3,
        out_specs=vmem,
        scratch_shapes=[
            pltpu.VMEM((4, half, width), BF16),
            pltpu.VMEM((4, half, width), BF16),
            pltpu.VMEM((2, half // 2, width), BF16),
            pltpu.VMEM((2, half, width), BF16),
            pltpu.VMEM((half, width), BF16),
            pltpu.VMEM((half, width), BF16),
            pltpu.VMEM(cot.shape, BF16),
            dma, dma((4,)), dma((4,)), dma((6,)), dma((6,)), dma, dma, dma((3,)), dma((3,)),
        ],
        compiler_params=pltpu.CompilerParams(collective_id=1, has_side_effects=True),
        name="give_back",
    )(part, target, cot)


def joined_along(blocks, dim):
    dims = list(blocks.shape[1:])
    dims[dim] *= blocks.shape[0]
    return jnp.moveaxis(blocks, 0, dim).reshape(dims)


def copy_for_each(shard, axis):
    copies = jnp.broadcast_to(shard, (lax.axis_size(axis), *shard.shape))
    return lax.all_to_all(copies, axis, split_axis=0, concat_axis=0, tiled=True)


def stacked_from(shard, axes, turns):
    blocks = shard
    for k in turns:
        blocks = lax.all_gather(blocks, axes[k])
    done = turns[::-1]
    back = [done.index(k) for k in range(len(axes))]
    blocks = blocks.transpose(*back, *range(len(axes), blocks.ndim))
    return blocks.reshape(-1, *shard.shape)


def gather_axes(shard, axes, turns, dim):
    return joined_along(stacked_from(shard, axes, turns), dim)


def gathered_once(shard, axis):
    leaves = jax.tree.leaves(shard)
    turns = sorted(range(len(leaves)), key=lambda k: -leaves[k].size)
    width = (1, *leaves[turns[0]].shape)[-1]
    lines = [
        jnp.pad(leaves[k].reshape(-1), (0, -leaves[k].size % width)).reshape(-1, width)
        for k in turns
    ]
    both, at, found = (copy_for_each(jnp.concatenate(lines), axis), 0, {})
    for k, line in zip(turns, lines):
        slab = both[:, at : at + len(line)].reshape(len(both), -1)
        found[k] = slab[:, : leaves[k].size].reshape(-1, *leaves[k].shape)
        at += len(line)
    numbers = iter(range(len(leaves)))
    return jax.tree.map(lambda _: found[next(numbers)], shard)


def joined_by_halves(pieces, combine):
    while len(jax.tree.leaves(pieces)[0]) > 1:
        pieces = jax.vmap(combine)(
            *(jax.tree.map(lambda part: part[side::2], pieces) for side in (0, 1))
        )
    return jax.tree.map(lambda part: part[0], pieces)


def entering(shard, axis, combine, identity):
    length, mine = (lax.axis_size(axis), lax.axis_index(axis))
    passed = jnp.arange(length) > mine

    def kept(part, zero, own):
        part = jnp.where(
            passed.reshape(-1, *(1 for _ in own.shape)), part, jnp.asarray(zero, own.dtype)
        )
        return part[::-1]

    pieces = gathered_once(shard, axis)
    return joined_by_halves(jax.tree.map(kept, pieces, identity, shard), combine)


def in_blocks(shard, dim, length):
    before, after = (shard.shape[:dim], shard.shape[dim + 1 :])
    return jnp.moveaxis(shard.reshape(*before, length, -1, *after), dim, 0)


def sent_and_summed(shard, axis, dim):
    blocks = in_blocks(shard, dim, lax.axis_size(axis))
    arrived = lax.all_to_all(blocks, axis, split_axis=0, concat_axis=0, tiled=True)
    return arrived.astype(jnp.float32).sum(axis=0)


def silu_slope(value):
    sig_value = jax.nn.sigmoid(value)
    return sig_value * (1.0 + value * (1.0 - sig_value))


def compose(upper_map, lower_map):
    return (lower_map[0] * upper_map[0], lower_map[1] + lower_map[0] * upper_map[1])


def chain_join(higher_map, lower_map):
    return (lower_map[0] * higher_map[0], lower_map[1] + lower_map[0] * higher_map[1])


def expert_backward(inputs, grads_in, gate_weight, up_weight, down_weight):
    gate_value = jnp.dot(inputs, gate_weight, preferred_element_type=jnp.float32)
    up_value = jnp.dot(inputs, up_weight, preferred_element_type=jnp.float32)
    active = jax.nn.silu(gate_value)
    hidden = (active * up_value).astype(jnp.bfloat16)
    down_grad = jnp.einsum(
        "rf,rd->fd", hidden, grads_in, preferred_element_type=jnp.float32
    ).astype(jnp.bfloat16)
    hidden_grad = jnp.einsum("rd,fd->rf", grads_in, down_weight, preferred_element_type=jnp.float32)
    gate_grad = (hidden_grad * up_value * silu_slope(gate_value)).astype(jnp.bfloat16)
    up_grad = (hidden_grad * active).astype(jnp.bfloat16)
    gate_weight_grad = jnp.einsum(
        "rd,rf->df", inputs, gate_grad, preferred_element_type=jnp.float32
    ).astype(jnp.bfloat16)
    up_weight_grad = jnp.einsum(
        "rd,rf->df", inputs, up_grad, preferred_element_type=jnp.float32
    ).astype(jnp.bfloat16)
    token_part = jnp.einsum("rf,df->rd", gate_grad, gate_weight, preferred_element_type=jnp.float32)
    token_part = token_part + jnp.einsum(
        "rf,df->rd", up_grad, up_weight, preferred_element_type=jnp.float32
    )
    return (gate_weight_grad, up_weight_grad, down_grad, token_part)


def local(
    result_cotangent_values,
    specialist_entry_vectors,
    chosen_specialists,
    specialist_mixing_shares,
    specialist_switch_maps,
    specialist_widen_maps,
    specialist_shrink_maps,
    memory_readout_map,
    memory_source_vectors,
    memory_hidden_values,
    feature_fading_speed,
    extra_log_fading,
    memory_switch_tiles,
    entry_switch_tiles,
):
    tok_rows, feature_count = result_cotangent_values.shape
    route_count = chosen_specialists.shape[1]
    sp_count = lax.axis_size(SP)
    expert_count = sp_count // SLICES
    capacity = min(tok_rows, 4 * tok_rows // expert_count)
    pairs = chosen_specialists.T.reshape(-1)
    order = (jnp.arange(tok_rows)[None, :] * route_count + jnp.arange(route_count)[:, None]).reshape(-1)
    earlier = (pairs[:, None] == pairs[None, :]) & (order[:, None] < order[None, :])
    target = pairs * capacity + jnp.sum(earlier.astype(jnp.int32), axis=0)
    dims = (lax.axis_size("sp_0"), lax.axis_size("sp_1"), lax.axis_size("tp"))
    both = dispatched(
        dims,
        capacity,
        target[None, :],
        specialist_mixing_shares,
        result_cotangent_values,
        specialist_entry_vectors,
    )
    gate_weight_grad, up_weight_grad, down_grad, token_part = expert_backward(
        both[0],
        both[1],
        specialist_switch_maps[0],
        specialist_widen_maps[0],
        specialist_shrink_maps[0],
    )
    mixed_grad = returned(
        dims,
        capacity,
        token_part.astype(jnp.bfloat16),
        target.reshape(route_count, tok_rows).T,
        result_cotangent_values,
    )
    col_count = memory_readout_map.shape[1]
    columns = mixed_grad
    upstream = jnp.dot(
        columns,
        gather_axes(memory_readout_map, (("sp_0", "sp_1"), "sp_2"), (0, 1), 0),
        preferred_element_type=jnp.float32,
    )
    blocks_here = memory_switch_tiles.shape[0]
    block_width = memory_switch_tiles.shape[1]
    blocks_in = memory_source_vectors.reshape(tok_rows, blocks_here, block_width)
    memory_switch_fraction = jax.nn.sigmoid(
        jnp.einsum(
            "tnc,ncd->tnd", blocks_in, memory_switch_tiles, preferred_element_type=jnp.float32
        ).reshape(tok_rows, col_count)
    )
    inp_open = jax.nn.sigmoid(
        jnp.einsum(
            "tnc,ncd->tnd", blocks_in, entry_switch_tiles, preferred_element_type=jnp.float32
        ).reshape(tok_rows, col_count)
    )
    xin = memory_source_vectors.astype(jnp.float32)
    log_fading_factor = (
        -8.0 * memory_switch_fraction * feature_fading_speed[None, :] + extra_log_fading[:, None]
    )
    decay_mult = jnp.exp(log_fading_factor)
    spare_room = -jnp.expm1(2.0 * log_fading_factor)
    in_scale = jnp.sqrt(jnp.maximum(spare_room, 0.01))
    drive = in_scale * inp_open * xin
    coeff = jnp.concatenate([decay_mult[1:], jnp.ones((1, col_count), jnp.float32)], axis=0)
    prod_after, local_part = lax.associative_scan(compose, (coeff, upstream), reverse=True, axis=0)
    alpha_part = decay_mult[0] * local_part[0]
    beta_part = decay_mult[0] * prod_after[0]
    carried = entering(
        (beta_part, alpha_part),
        SP,
        chain_join,
        (jnp.ones_like(beta_part), jnp.zeros_like(alpha_part)),
    )
    incoming = carried[1]
    dstate = local_part + prod_after * incoming[None, :]
    scale_slope = jnp.where(spare_room > 0.01, -decay_mult * decay_mult / in_scale, 0.0)
    log_grad = dstate * (
        memory_hidden_values.astype(jnp.float32) - drive + scale_slope * inp_open * xin
    )
    grad_rec = (
        log_grad
        * (-8.0 * feature_fading_speed[None, :])
        * memory_switch_fraction
        * (1.0 - memory_switch_fraction)
    ).astype(jnp.bfloat16)
    grad_in = (dstate * in_scale * xin * inp_open * (1.0 - inp_open)).astype(jnp.bfloat16)
    back_rec = jnp.einsum(
        "tnd,ncd->tnc",
        grad_rec.reshape(tok_rows, blocks_here, block_width),
        memory_switch_tiles,
        preferred_element_type=jnp.float32,
    )
    back_in = jnp.einsum(
        "tnd,ncd->tnc",
        grad_in.reshape(tok_rows, blocks_here, block_width),
        entry_switch_tiles,
        preferred_element_type=jnp.float32,
    )
    lru_input_grad = (
        dstate * in_scale * inp_open
        + back_rec.reshape(tok_rows, col_count)
        + back_in.reshape(tok_rows, col_count)
    )
    columns = mixed_grad
    out_proj_grad = sent_and_summed(
        jnp.einsum(
            "tr,tc->rc", columns, memory_hidden_values, preferred_element_type=jnp.float32
        ).astype(jnp.bfloat16),
        SP,
        0,
    )
    return (
        gate_weight_grad[None],
        up_weight_grad[None],
        down_grad[None],
        out_proj_grad,
        lru_input_grad,
    )


def solution(mesh):
    finer = Mesh(mesh.devices.reshape(8, 4, 2, mesh.shape["tp"]), ("sp_0", "sp_1", "sp_2", "tp"))
    in_specs = (
        P(SP, None),
        P(SP, None),
        P(SP, None),
        P(SP, None),
        P(SP, None, "tp"),
        P(SP, None, "tp"),
        P(SP, "tp", None),
        P(SP, "tp"),
        P(SP, "tp"),
        P(SP, "tp"),
        P("tp"),
        P(SP),
        P("tp", None, None),
        P("tp", None, None),
    )
    out_specs = (P(SP, None, "tp"), P(SP, None, "tp"), P(SP, "tp", None), P(SP, "tp"), P(SP, "tp"))
    return jax.shard_map(local, mesh=finer, in_specs=in_specs, out_specs=out_specs, check_vma=False)
```

```python
import functools

import jax
import jax.numpy as jnp
from jax import lax
from jax.experimental import pallas as pl
from jax.experimental.pallas import tpu as pltpu
from jax.sharding import Mesh
from jax.sharding import PartitionSpec as P

SLICES = 2
SP = ("sp_0", "sp_1", "sp_2")
MESH = pl.DeviceIdType.MESH
F32, BF16 = jnp.float32, jnp.bfloat16


def place():
    return tuple(lax.axis_index(n) for n in ("sp_0", "sp_1", "sp_2", "tp"))


def offset_of(k, count):
    odd = lax.rem(k, 2)
    return lax.rem(odd * ((k + 1) // 2) + (1 - odd) * (count - k // 2), count)


def greet_peers(dims, far_share):
    nz, nx, ny = dims
    z, x, c, y = place()
    barrier = pltpu.get_barrier_semaphore()

    def greet(i, _):
        to = (lax.rem(z + i // nx, nz), lax.rem(x + lax.rem(i, nx), nx), c, y)
        pl.semaphore_signal(barrier, inc=1, device_id=to, device_id_type=MESH)
        return 0

    lax.fori_loop(1, nz * nx, greet, 0)
    steps = (1, 2, 3) if far_share else (1, 3)
    for step in steps:
        to = (z, x, c, lax.rem(y + step, ny))
        pl.semaphore_signal(barrier, inc=1, device_id=to, device_id_type=MESH)
    pl.semaphore_signal(barrier, inc=1, device_id=(z, x, 1 - c, y), device_id_type=MESH)
    return barrier, nz * nx - 1 + len(steps) + 1


def drained(ref, sem):
    pltpu.make_async_copy(ref, ref, sem).wait()


def dispatch_kernel(
    dims, cap, target, share, cot, rows, out, slots, own_sem, d_send, d_recv, y_send, y_recv,
    f_send, f_recv, c_send, c_recv,
):
    nz, nx, ny = dims
    z, x, c, y = place()
    barrier, greetings = greet_peers(dims, False)
    width = cot.shape[1] // ny
    half = nz * nx * cap
    group = nx * cap
    cols = pl.ds(pl.multiple_of(y * width, 128), width)

    slot = lax.broadcasted_iota(jnp.int32, (half, target.shape[1]), 0)
    onehot = jnp.where(slot == target[...], 1.0, 0.0).astype(BF16)
    some = rows[:, cols]
    slots[0] = jnp.dot(
        onehot, jnp.concatenate([some, some], axis=0), preferred_element_type=F32
    ).astype(BF16)
    some = cot[:, cols].astype(F32)
    scaled = [(share[:, k : k + 1] * some).astype(BF16) for k in range(2)]
    slots[1] = jnp.dot(
        onehot, jnp.concatenate(scaled, axis=0), preferred_element_type=F32
    ).astype(BF16)

    pl.semaphore_wait(barrier, greetings)

    def source(e):
        return slots.at[:, pl.ds(pl.multiple_of(e * cap, cap), cap), :]

    def target_rows(k):
        start = pl.multiple_of(c * half + (k * nx + x) * cap, cap)
        return out.at[:, pl.ds(start, cap), cols]

    own = pltpu.make_async_copy(source(z * nx + x), target_rows(0), own_sem)
    own.start()

    def push(i, _):
        k, dx = i // nx, lax.rem(i, nx)
        tz, tx = lax.rem(z + offset_of(k, nz), nz), lax.rem(x + dx, nx)
        pltpu.make_async_remote_copy(
            src_ref=source(tz * nx + tx),
            dst_ref=target_rows(k),
            send_sem=d_send,
            recv_sem=d_recv.at[k],
            device_id=(tz, tx, c, y),
            device_id_type=MESH,
        ).start()
        return 0

    lax.fori_loop(1, nz * nx, push, 0)

    def block(k, turn):
        start = pl.multiple_of(c * half + k * group, cap)
        share_of = lax.rem(y + turn, ny)
        return out.at[
            :, pl.ds(start, group), pl.ds(pl.multiple_of(share_of * width, 128), width)
        ]

    def across(k, turn):
        pltpu.make_async_remote_copy(
            src_ref=block(k, turn),
            dst_ref=block(k, turn),
            send_sem=c_send,
            recv_sem=c_recv,
            device_id=(z, x, 1 - c, y),
            device_id_type=MESH,
        ).start()

    def along(k, turn, step, send, recv):
        copy = pltpu.make_async_remote_copy(
            src_ref=block(k, turn),
            dst_ref=block(k, turn),
            send_sem=send,
            recv_sem=recv,
            device_id=(z, x, c, lax.rem(y + step, ny)),
            device_id_type=MESH,
        )
        copy.start()

    for turn in range(nz + 3):
        k = turn
        if k < nz:
            if k == 0:
                drained(slots.at[:, pl.ds(0, group - cap), :], d_recv.at[0])
                own.wait()
            else:
                drained(block(k, 0), d_recv.at[k])
            along(k, 0, 1, y_send.at[0, k], y_recv.at[0, k])
            along(k, 0, 3, y_send.at[1, k], y_recv.at[1, k])
            across(k, 0)
        k = turn - 2
        if 0 <= k < nz:
            drained(block(k, 3), y_recv.at[0, k])
            if k % 2 == 0:
                along(k, 3, 1, f_send.at[k], f_recv.at[k])
            across(k, 3)
            drained(block(k, 1), y_recv.at[1, k])
            if k % 2 == 1:
                along(k, 1, 3, f_send.at[k], f_recv.at[k])
            across(k, 1)
        k = turn - 3
        if 0 <= k < nz:
            drained(block(k, 2), f_recv.at[k])
            across(k, 2)

    whole = out.at[:, pl.ds(pl.multiple_of((1 - c) * half, cap), half), :]
    drained(whole, c_recv)
    drained(whole, c_send)
    drained(slots.at[:, pl.ds(0, half - cap), :], d_send)
    for k in range(nz):
        drained(block(k, 0), y_send.at[0, k])
        drained(block(k, 0), y_send.at[1, k])
        drained(block(k, 2), f_send.at[k])


def dispatched(dims, cap, target, share, cot, rows):
    nz, nx, ny = dims
    half = nz * nx * cap
    vmem = pl.BlockSpec(memory_space=pltpu.VMEM)
    dma = pltpu.SemaphoreType.DMA
    return pl.pallas_call(
        functools.partial(dispatch_kernel, dims, cap),
        out_shape=jax.ShapeDtypeStruct((2, 2 * half, cot.shape[1]), BF16),
        in_specs=[vmem] * 4,
        out_specs=pl.BlockSpec(memory_space=pl.ANY),
        scratch_shapes=[
            pltpu.VMEM((2, half, cot.shape[1] // ny), BF16),
            dma, dma, dma((nz,)), dma((2, nz)), dma((2, nz)), dma((nz,)), dma((nz,)), dma, dma,
        ],
        compiler_params=pltpu.CompilerParams(collective_id=0, has_side_effects=True),
        name="dispatch",
    )(target, share, cot, rows)


def return_kernel(
    dims, cap, part, target, cot, rmap, xmem, hid, fade, extra, rtile, itile, both, acts3,
    gate_out, up_out, down_out, proj_out, lru_out,
    pair, sums, far, near, back, mine, moe, mixed, xy, acts, grads, wide, held, turned, cross,
    fold, rest, levels, pieces, alphas, betas, weights, small,
    own_sem, p_send, p_recv, y_send, y_recv, r_send, r_recv, m_send, m_recv, in_sem, out_sem,
    b_send, b_recv, z_send, z_recv, s_send, s_recv, h_send, h_recv, t_send, t_recv, a_send, a_recv,
    g_send, g_recv, q_send, q_recv,
):
    nz, nx, ny = dims
    z, x, c, y = place()
    plane = nz * nx * 2
    index = (z * nx + x) * 2 + c
    width = cot.shape[1] // ny
    toks = cot.shape[0]
    half = nz * nx * cap
    mid = half // 2
    barrier = pltpu.get_barrier_semaphore()

    def sp_at(i):
        i = lax.rem(index + i, plane)
        return (i // (2 * nx), lax.rem(i // 2, nx), lax.rem(i, 2), y)

    def greet(i, _):
        pl.semaphore_signal(barrier, inc=1, device_id=sp_at(i), device_id_type=MESH)
        return 0

    lax.fori_loop(1, plane, greet, 0)
    for step in (1, 2, 3):
        to = (z, x, c, lax.rem(y + step, ny))
        pl.semaphore_signal(barrier, inc=1, device_id=to, device_id_type=MESH)

    loads = [pltpu.make_async_copy(both, xy, in_sem.at[0])]
    for m in range(3):
        loads.append(pltpu.make_async_copy(acts3[m], acts.at[m], in_sem.at[m + 1]))
    for load in loads:
        load.start()
    wide[z, x, c] = rmap[...]
    held[x, c] = hid[...]
    pl.semaphore_wait(barrier, plane - 1 + 3)

    def cols(turn):
        return pl.ds(pl.multiple_of(lax.rem(y + turn, ny) * width, 128), width)

    def remote(src, dst, send, recv, to):
        pltpu.make_async_remote_copy(
            src_ref=src, dst_ref=dst, send_sem=send, recv_sem=recv, device_id=to,
            device_id_type=MESH,
        ).start()

    other = (z, x, 1 - c, y)
    theirs = pl.ds(pl.multiple_of((1 - c) * half, cap), half)
    ours = pl.multiple_of(c * half, cap)
    for turn in (2, 1, 3, 0):
        remote(
            part.at[theirs, cols(turn)], pair.at[turn], p_send.at[turn], p_recv.at[turn], other
        )
    for step in range(1, nx):
        to = (z, lax.rem(x + step, nx), c, y)
        remote(rmap, wide.at[z, x, c], b_send.at[step - 1], b_recv.at[step - 1], to)
    for step in range(1, nx):
        to = (z, lax.rem(x + step, nx), c, y)
        remote(hid, held.at[x, c], h_send.at[step - 1], h_recv.at[step - 1], to)

    chunk = 256

    def weight_grad(m):
        def some(i, _):
            here = pl.ds(pl.multiple_of(i * chunk, chunk), chunk)
            grads[m, :, here] = jnp.dot(
                acts[m], xy[m // 2, :, here], preferred_element_type=F32
            ).astype(BF16)
            return 0

        lax.fori_loop(0, cot.shape[1] // chunk, some, 0)
        pltpu.make_async_copy(
            grads.at[m], (gate_out, up_out, down_out)[m], out_sem.at[m]
        ).start()

    rounds = nz // 2

    def ring_block(s, side):
        away = nz - s if side == 0 else s
        from_z = lax.rem(z + away, nz)
        if s < rounds:
            return wide.at[from_z, :, c]
        return wide.at[from_z, pl.ds(side * (nx // 2), nx // 2), c]

    def ring_sent(s, side):
        away = nz - s if side == 0 else s
        from_z = lax.rem(z + away, nz)
        if s < rounds - 1:
            return wide.at[from_z, :, c]
        return wide.at[from_z, pl.ds(side * (nx // 2), nx // 2), c]

    def ring(s):
        if s == 0:
            for step in range(1, nx):
                drained(rmap, b_recv.at[step - 1])
            remote(wide.at[z, :, c], wide.at[z, :, c], s_send, s_recv, other)
        else:
            for side in range(2):
                drained(ring_block(s, side), z_recv.at[side, s - 1])
                remote(ring_block(s, side), ring_block(s, side), s_send, s_recv, other)
        if s < rounds:
            for side in range(2):
                to = (lax.rem(z + (1 if side == 0 else nz - 1), nz), x, c, y)
                some = ring_sent(s, side)
                remote(some, some, z_send.at[side, s], z_recv.at[side, s], to)

    loads[0].wait()
    loads[1].wait()
    weight_grad(0)
    ring(0)
    for step in range(1, nx):
        drained(hid, h_recv.at[step - 1])
    remote(held.at[:, c], held.at[:, c], t_send, t_recv, other)

    up, down = (z, x, c, lax.rem(y + 1, ny)), (z, x, c, lax.rem(y + 3, ny))
    low, high = pl.ds(0, mid), pl.ds(mid, mid)

    def added(turn):
        drained(pair.at[turn], p_recv.at[turn])

        def some(i, _):
            here = pl.multiple_of(i * 64, 64)
            total = part[pl.ds(ours + here, 64), cols(turn)].astype(F32)
            total = total + pair[turn, pl.ds(here, 64), :].astype(F32)
            sums[turn, pl.ds(here, 64), :] = total.astype(BF16)
            return 0

        lax.fori_loop(0, half // 64, some, 0)

    added(2)
    remote(sums.at[2, low], far.at[0], y_send.at[0], y_recv.at[0], up)
    remote(sums.at[2, high], far.at[1], y_send.at[1], y_recv.at[1], down)
    added(1)
    remote(sums.at[1, high], near.at[0, high], y_send.at[2], y_recv.at[2], up)
    added(3)
    remote(sums.at[3, low], near.at[1, low], y_send.at[3], y_recv.at[3], down)
    added(0)

    blocks, span = rtile.shape[0], rtile.shape[1]
    for b in range(blocks):
        here = pl.ds(b * span, span)
        some = xmem[:, here]
        rec = jax.nn.sigmoid(jnp.dot(some, rtile[b], preferred_element_type=F32))
        inp = jax.nn.sigmoid(jnp.dot(some, itile[b], preferred_element_type=F32))
        speed = -8.0 * fade[:, here]
        log_decay = rec * speed + extra[...]
        decay = jnp.exp(log_decay)
        spare = 1.0 - jnp.exp(2.0 * log_decay)
        scale = jnp.sqrt(jnp.maximum(spare, 0.01))
        gated = inp * some.astype(F32)
        slope = jnp.where(spare > 0.01, -decay * decay / scale, 0.0)
        level = hid[:, here].astype(F32) - scale * gated + slope * gated
        pieces[0, :, here] = level * speed * rec * (1.0 - rec)
        pieces[1, :, here] = scale * gated * (1.0 - inp)
        pieces[2, :, here] = scale * inp
        pieces[4, :, here] = decay
    row = lax.broadcasted_iota(jnp.int32, (toks, 128), 0)
    reach = [1 << s for s in range(toks.bit_length() - 1)]

    def products(i, _):
        here = pl.ds(pl.multiple_of(i * 128, 128), 128)
        decay = pieces[4, :, here]
        prod = jnp.where(row < toks - 1, pltpu.roll(decay, toks - 1, 0), 1.0)
        for n, s in enumerate(reach):
            inside = row < toks - s
            levels[n, :, here] = jnp.where(inside, prod, 0.0)
            prod = prod * jnp.where(inside, pltpu.roll(prod, toks - s, 0), 1.0)
        pieces[3, :, here] = prod
        small[0, pl.ds(i, 1), :] = decay[0:1] * prod[0:1]
        return 0

    for i in range(width // 128):
        products(i, 0)
    betas[index] = small[0]

    def tell(src, dst, send, recv):
        def one(i, _):
            remote(src, dst.at[index], send, recv, sp_at(i))
            return 0

        lax.fori_loop(1, plane, one, 0)

    tell(small.at[0], betas, a_send.at[0], a_recv.at[0])

    ring(1)

    def joined(side, turn, first):
        drained(far.at[side], y_recv.at[side])

        def some(i, _):
            here = pl.multiple_of(i * 64, 64)
            total = sums[turn, pl.ds(first + here, 64), :].astype(F32)
            total = total + far[side, pl.ds(here, 64), :].astype(F32)
            sums[turn, pl.ds(first + here, 64), :] = total.astype(BF16)
            return 0

        lax.fori_loop(0, mid // 64, some, 0)

    joined(0, 1, 0)
    remote(sums.at[1, low], near.at[0, low], y_send.at[4], y_recv.at[4], up)
    joined(1, 3, mid)
    remote(sums.at[3, high], near.at[1, high], y_send.at[5], y_recv.at[5], down)

    ring(2)
    loads[2].wait()
    weight_grad(1)
    for s in range(3, rounds + 1):
        ring(s)

    drained(betas.at[pl.ds(0, plane - 1)], a_recv.at[0])

    def weigh(j, run):
        later = j > index
        weights[j] = jnp.where(later, run, 0.0)
        return jnp.where(later, run * betas[j], 1.0)

    lax.fori_loop(0, plane, weigh, jnp.ones((width // 128, 128), F32))

    me = z * nx + x

    def finished(first, early, late):
        drained(far.at[0], y_recv.at[early])
        drained(far.at[0], y_recv.at[late])

        def some(i, _):
            here = pl.multiple_of(first + i * 64, 64)
            total = sums[0, pl.ds(here, 64), :].astype(F32)
            total = total + near[0, pl.ds(here, 64), :].astype(F32)
            total = total + near[1, pl.ds(here, 64), :].astype(F32)
            mine[pl.ds(here, 64), :] = total.astype(BF16)
            return 0

        lax.fori_loop(0, mid // 64, some, 0)

    def give(i, _):
        k, sx = i // nx, lax.rem(i, nx)
        sx = lax.rem(x + sx, nx)
        to = (lax.rem(z + nz - offset_of(k, nz), nz), sx, c, y)
        remote(
            mine.at[pl.ds(pl.multiple_of((k * nx + sx) * cap, cap), cap), :],
            back.at[pl.ds(pl.multiple_of(me * cap, cap), cap), :],
            r_send, r_recv, to,
        )
        return 0

    finished(mid, 2, 5)
    lax.fori_loop(nz * nx // 2, nz * nx, give, 0)
    finished(0, 4, 3)
    back[pl.ds(pl.multiple_of(me * cap, cap), cap), :] = mine[
        pl.ds(pl.multiple_of(x * cap, cap), cap), :
    ]
    lax.fori_loop(1, nz * nx // 2, give, 0)

    loads[3].wait()
    weight_grad(2)
    slot = lax.broadcasted_iota(jnp.int32, (toks, half), 1)
    chosen = (slot == target[:, 0:1]) | (slot == target[:, 1:2])
    onehot = jnp.where(chosen, 1.0, 0.0).astype(BF16)
    drained(back.at[pl.ds(0, half - cap), :], r_recv)
    moe[:, cols(0)] = jnp.dot(onehot, back[...], preferred_element_type=F32).astype(BF16)
    for step in (1, 3, 2):
        remote(
            moe.at[:, cols(0)], moe.at[:, cols(0)], m_send.at[step - 1], m_recv.at[step - 1],
            (z, x, c, lax.rem(y + step, ny)),
        )
    for step in (1, 3, 2):
        drained(moe.at[:, cols(ny - step)], m_recv.at[step - 1])
    mixed[...] = (cot[...].astype(F32) + moe[...].astype(F32)).astype(BF16)

    lines = rmap.shape[0]
    turned[...] = jnp.transpose(mixed[...]).reshape(nz, 2 * nx, lines, toks)
    spot = x * 2 + c
    cross[:, :, pl.ds(pl.multiple_of(spot * toks, toks), toks)] = turned[:, spot]

    for step in range(1, 2 * nx):
        to = lax.rem(spot + step, 2 * nx)
        remote(
            turned.at[:, to],
            cross.at[:, :, pl.ds(pl.multiple_of(spot * toks, toks), toks)],
            g_send.at[step - 1], g_recv.at[step - 1],
            (z, to // 2, lax.rem(to, 2), y),
        )

    drained(wide.at[:, :, 1 - c], s_recv)
    state = jnp.dot(
        mixed[...], wide[...].reshape(-1, width), preferred_element_type=F32
    )
    for n, s in enumerate(reach):
        state = state + levels[n] * pltpu.roll(state, toks - s, 0)
    first = pieces[4, 0:1, :] * state[0:1]
    for i in range(width // 128):
        small[1, pl.ds(i, 1), :] = first[:, i * 128 : (i + 1) * 128]
    alphas[index] = small[1]
    tell(small.at[1], alphas, a_send.at[1], a_recv.at[1])

    drained(held.at[:, 1 - c], t_recv)
    for step in range(1, 2 * nx):
        drained(turned.at[:, 0], g_recv.at[step - 1])
    total = jnp.dot(
        cross[...].reshape(nz * lines, 2 * nx * toks),
        held[...].reshape(2 * nx * toks, width),
        preferred_element_type=F32,
    )
    fold[...] = total.astype(BF16).reshape(nz, lines, width)
    rest[z] = fold[z]
    for step in range(1, nz):
        to = lax.rem(z + step, nz)
        remote(fold.at[to], rest.at[z], q_send.at[step - 1], q_recv.at[step - 1], (to, x, c, y))

    drained(alphas.at[pl.ds(0, plane - 1)], a_recv.at[1])
    carried = jnp.sum(weights[...] * alphas[...], axis=0)
    carried = jnp.concatenate([carried[i : i + 1] for i in range(width // 128)], axis=1)
    state = state + pieces[3] * carried
    grad_rec = (state * pieces[0]).astype(BF16)
    grad_in = (state * pieces[1]).astype(BF16)
    direct = state * pieces[2]
    turn_dims = (((1,), (1,)), ((), ()))
    for b in range(blocks):
        here = slice(b * span, (b + 1) * span)
        lru_out[:, here] = (
            direct[:, here]
            + lax.dot_general(grad_rec[:, here], rtile[b], turn_dims, preferred_element_type=F32)
            + lax.dot_general(grad_in[:, here], itile[b], turn_dims, preferred_element_type=F32)
        )

    for step in range(1, nz):
        drained(fold.at[0], q_recv.at[step - 1])
    summed = rest[0].astype(F32)
    for i in range(1, nz):
        summed = summed + rest[i].astype(F32)
    proj_out[...] = summed

    for turn in range(4):
        drained(pair.at[turn], p_send.at[turn])
    for i in range(6):
        drained(far.at[0], y_send.at[i])
    drained(back.at[pl.ds(0, half - cap), :], r_send)
    for step in (1, 2, 3):
        drained(moe.at[:, cols(0)], m_send.at[step - 1])
    for step in range(nx - 1):
        drained(rmap, b_send.at[step])
        drained(hid, h_send.at[step])
    for s in range(rounds):
        for side in range(2):
            drained(ring_sent(s, side), z_send.at[side, s])
    drained(wide.at[:, :, c], s_send)
    drained(held.at[:, c], t_send)
    for i in range(2):
        drained(betas.at[pl.ds(0, plane - 1)], a_send.at[i])
    for step in range(2 * nx - 1):
        drained(turned.at[:, 0], g_send.at[step])
    for step in range(nz - 1):
        drained(fold.at[0], q_send.at[step])
    for m in range(3):
        pltpu.make_async_copy(
            grads.at[m], (gate_out, up_out, down_out)[m], out_sem.at[m]
        ).wait()


def return_entry(dims, cap, *refs):
    return_kernel(dims, cap, *refs[:11], refs[11:14], *refs[14:])


def returned(dims, cap, part, target, cot, rmap, xmem, hid, fade, extra, rtile, itile, both, acts):
    nz, nx, ny = dims
    half, width = nz * nx * cap, cot.shape[1] // ny
    toks, feats = cot.shape
    lines, units = rmap.shape[0], acts[0].shape[0]
    plane, lanes, steps = nz * nx * 2, width // 128, toks.bit_length() - 1
    vmem, anyw = pl.BlockSpec(memory_space=pltpu.VMEM), pl.BlockSpec(memory_space=pl.ANY)
    dma = pltpu.SemaphoreType.DMA
    return pl.pallas_call(
        functools.partial(return_entry, dims, cap),
        out_shape=[jax.ShapeDtypeStruct((units, feats), BF16)] * 3
        + [
            jax.ShapeDtypeStruct((lines, width), F32),
            jax.ShapeDtypeStruct((toks, width), F32),
        ],
        in_specs=[vmem] * 10 + [anyw] * 4,
        out_specs=[anyw] * 3 + [vmem] * 2,
        scratch_shapes=[
            pltpu.VMEM((4, half, width), BF16),
            pltpu.VMEM((4, half, width), BF16),
            pltpu.VMEM((2, half // 2, width), BF16),
            pltpu.VMEM((2, half, width), BF16),
            pltpu.VMEM((half, width), BF16),
            pltpu.VMEM((half, width), BF16),
            pltpu.VMEM((toks, feats), BF16),
            pltpu.VMEM((toks, feats), BF16),
            pltpu.VMEM(both.shape, BF16),
            pltpu.VMEM((3,) + acts[0].shape, BF16),
            pltpu.VMEM((3, units, feats), BF16),
            pltpu.VMEM((nz, nx, 2, lines, width), BF16),
            pltpu.VMEM((nx, 2, toks, width), BF16),
            pltpu.VMEM((nz, 2 * nx, lines, toks), BF16),
            pltpu.VMEM((nz, lines, 2 * nx * toks), BF16),
            pltpu.VMEM((nz, lines, width), BF16),
            pltpu.VMEM((nz, lines, width), BF16),
            pltpu.VMEM((steps, toks, width), F32),
            pltpu.VMEM((5, toks, width), F32),
            pltpu.VMEM((plane, lanes, 128), F32),
            pltpu.VMEM((plane, lanes, 128), F32),
            pltpu.VMEM((plane, lanes, 128), F32),
            pltpu.VMEM((2, lanes, 128), F32),
            dma, dma((4,)), dma((4,)), dma((6,)), dma((6,)), dma, dma, dma((3,)), dma((3,)),
            dma((4,)), dma((3,)), dma((nx - 1,)), dma((nx - 1,)), dma((2, nz // 2)),
            dma((2, nz // 2)), dma, dma, dma((nx - 1,)), dma((nx - 1,)), dma, dma, dma((2,)),
            dma((2,)), dma((2 * nx - 1,)), dma((2 * nx - 1,)), dma((nz - 1,)), dma((nz - 1,)),
        ],
        compiler_params=pltpu.CompilerParams(
            collective_id=1, has_side_effects=True, vmem_limit_bytes=60 * 2**20
        ),
        name="give_back",
    )(part, target, cot, rmap, xmem, hid, fade, extra, rtile, itile, both, *acts)


def silu_slope(value):
    sig_value = jax.nn.sigmoid(value)
    return sig_value * (1.0 + value * (1.0 - sig_value))


def expert_backward(inputs, grads_in, gate_weight, up_weight, down_weight):
    gate_value = jnp.dot(inputs, gate_weight, preferred_element_type=jnp.float32)
    up_value = jnp.dot(inputs, up_weight, preferred_element_type=jnp.float32)
    active = jax.nn.silu(gate_value)
    hidden = (active * up_value).astype(jnp.bfloat16)
    hidden_grad = jnp.einsum("rd,fd->rf", grads_in, down_weight, preferred_element_type=jnp.float32)
    gate_grad = (hidden_grad * up_value * silu_slope(gate_value)).astype(jnp.bfloat16)
    up_grad = (hidden_grad * active).astype(jnp.bfloat16)
    token_part = jnp.einsum("rf,df->rd", gate_grad, gate_weight, preferred_element_type=jnp.float32)
    token_part = token_part + jnp.einsum(
        "rf,df->rd", up_grad, up_weight, preferred_element_type=jnp.float32
    )
    return gate_grad.T, up_grad.T, hidden.T, token_part.astype(jnp.bfloat16)


def local(
    result_cotangent_values,
    specialist_entry_vectors,
    chosen_specialists,
    specialist_mixing_shares,
    specialist_switch_maps,
    specialist_widen_maps,
    specialist_shrink_maps,
    memory_readout_map,
    memory_source_vectors,
    memory_hidden_values,
    feature_fading_speed,
    extra_log_fading,
    memory_switch_tiles,
    entry_switch_tiles,
):
    tok_rows, feature_count = result_cotangent_values.shape
    route_count = chosen_specialists.shape[1]
    sp_count = lax.axis_size(SP)
    expert_count = sp_count // SLICES
    capacity = min(tok_rows, 4 * tok_rows // expert_count)
    pairs = chosen_specialists.T.reshape(-1)
    order = (jnp.arange(tok_rows)[None, :] * route_count + jnp.arange(route_count)[:, None]).reshape(-1)
    earlier = (pairs[:, None] == pairs[None, :]) & (order[:, None] < order[None, :])
    target = pairs * capacity + jnp.sum(earlier.astype(jnp.int32), axis=0)
    dims = (lax.axis_size("sp_0"), lax.axis_size("sp_1"), lax.axis_size("tp"))
    both = dispatched(
        dims,
        capacity,
        target[None, :],
        specialist_mixing_shares,
        result_cotangent_values,
        specialist_entry_vectors,
    )
    *acts, token_part = expert_backward(
        both[0],
        both[1],
        specialist_switch_maps[0],
        specialist_widen_maps[0],
        specialist_shrink_maps[0],
    )
    gate_weight_grad, up_weight_grad, down_grad, out_proj_grad, lru_input_grad = returned(
        dims,
        capacity,
        token_part,
        target.reshape(route_count, tok_rows).T,
        result_cotangent_values,
        memory_readout_map,
        memory_source_vectors,
        memory_hidden_values,
        feature_fading_speed[None, :],
        extra_log_fading[:, None],
        memory_switch_tiles,
        entry_switch_tiles,
        both,
        acts,
    )
    return (
        gate_weight_grad.T[None],
        up_weight_grad.T[None],
        down_grad[None],
        out_proj_grad,
        lru_input_grad,
    )


def solution(mesh):
    finer = Mesh(mesh.devices.reshape(8, 4, 2, mesh.shape["tp"]), ("sp_0", "sp_1", "sp_2", "tp"))
    in_specs = (
        P(SP, None),
        P(SP, None),
        P(SP, None),
        P(SP, None),
        P(SP, None, "tp"),
        P(SP, None, "tp"),
        P(SP, "tp", None),
        P(SP, "tp"),
        P(SP, "tp"),
        P(SP, "tp"),
        P("tp"),
        P(SP),
        P("tp", None, None),
        P("tp", None, None),
    )
    out_specs = (P(SP, None, "tp"), P(SP, None, "tp"), P(SP, "tp", None), P(SP, "tp"), P(SP, "tp"))
    return jax.shard_map(local, mesh=finer, in_specs=in_specs, out_specs=out_specs, check_vma=False)
```

```python
import functools

import jax
import jax.numpy as jnp
from jax import lax
from jax.experimental import pallas as pl
from jax.experimental.pallas import tpu as pltpu
from jax.sharding import Mesh
from jax.sharding import PartitionSpec as P

SLICES = 2
SP = ("sp_0", "sp_1", "sp_2")
MESH = pl.DeviceIdType.MESH
F32, BF16 = jnp.float32, jnp.bfloat16


def place():
    return tuple(lax.axis_index(n) for n in ("sp_0", "sp_1", "sp_2", "tp"))


def offset_of(k, count):
    odd = lax.rem(k, 2)
    return lax.rem(odd * ((k + 1) // 2) + (1 - odd) * (count - k // 2), count)


def drained(ref, sem):
    pltpu.make_async_copy(ref, ref, sem).wait()


def layer_kernel(
    dims, cap, target, spots, share, cot, rows, rmap, xmem, hid, fade, extra, rtile, itile, maps,
    outs, proj_out, lru_out,
    slots, xy, wts, accs, acts, give_rows, own_rows, pair, sums, far, near, back, mine, moe, mixed,
    grads, wide, held, turned, cross, fold, rest, levels, pieces, alphas, betas, weights, small,
    own_sem, in_sem, out_sem, d_send, d_recv, y_send, y_recv, f_send, f_recv, c_send, c_recv,
    p_send, p_recv, e_send, e_recv, r_send, r_recv, m_send, m_recv, b_send, b_recv, z_send, z_recv,
    s_send, s_recv, h_send, h_recv, t_send, t_recv, a_send, a_recv, g_send, g_recv, q_send, q_recv,
):
    nz, nx, ny = dims
    z, x, c, y = place()
    plane = nz * nx * 2
    index = (z * nx + x) * 2 + c
    me = z * nx + x
    toks, feats = cot.shape
    width = feats // ny
    half = nz * nx * cap
    group = nx * cap
    other = (z, x, 1 - c, y)
    up, down = (z, x, c, lax.rem(y + 1, ny)), (z, x, c, lax.rem(y + 3, ny))
    barrier = pltpu.get_barrier_semaphore()

    def sp_at(i):
        i = lax.rem(index + i, plane)
        return (i // (2 * nx), lax.rem(i // 2, nx), lax.rem(i, 2), y)

    def greet(i, _):
        pl.semaphore_signal(barrier, inc=1, device_id=sp_at(i), device_id_type=MESH)
        return 0

    lax.fori_loop(1, plane, greet, 0)
    for step in (1, 2, 3):
        to = (z, x, c, lax.rem(y + step, ny))
        pl.semaphore_signal(barrier, inc=1, device_id=to, device_id_type=MESH)

    def cols(turn):
        return pl.ds(pl.multiple_of(lax.rem(y + turn, ny) * width, 128), width)

    def remote(src, dst, send, recv, to):
        pltpu.make_async_remote_copy(
            src_ref=src, dst_ref=dst, send_sem=send, recv_sem=recv, device_id=to,
            device_id_type=MESH,
        ).start()

    loads = [pltpu.make_async_copy(maps[m], wts.at[m], in_sem.at[m]) for m in range(3)]
    for load in loads:
        load.start()
    wide[z, x, c] = rmap[...]
    held[x, c] = hid[...]

    slot = lax.broadcasted_iota(jnp.int32, (half, target.shape[1]), 0)
    onehot = jnp.where(slot == target[...], 1.0, 0.0).astype(BF16)
    some = rows[:, cols(0)]
    slots[0] = jnp.dot(
        onehot, jnp.concatenate([some, some], axis=0), preferred_element_type=F32
    ).astype(BF16)
    some = cot[:, cols(0)].astype(F32)
    scaled = [(share[:, k : k + 1] * some).astype(BF16) for k in range(2)]
    slots[1] = jnp.dot(
        onehot, jnp.concatenate(scaled, axis=0), preferred_element_type=F32
    ).astype(BF16)

    def source(e):
        return slots.at[:, pl.ds(pl.multiple_of(e * cap, cap), cap), :]

    def landing(k):
        start = pl.multiple_of(c * half + (k * nx + x) * cap, cap)
        return xy.at[:, pl.ds(start, cap), cols(0)]

    here = pl.ds(pl.multiple_of(c * half + x * cap, cap), cap)
    mine_too = pl.ds(pl.multiple_of(me * cap, cap), cap)
    for i in range(2):
        xy[i, here, cols(0)] = slots[i, mine_too, :]
    pl.semaphore_wait(barrier, plane - 1 + 3)

    def push(i, _):
        k, dx = i // nx, lax.rem(i, nx)
        tz, tx = lax.rem(z + offset_of(k, nz), nz), lax.rem(x + dx, nx)
        remote(source(tz * nx + tx), landing(k), d_send, d_recv.at[k], (tz, tx, c, y))
        return 0

    lax.fori_loop(1, nz * nx, push, 0)
    for step in range(1, nx):
        to = (z, lax.rem(x + step, nx), c, y)
        remote(rmap, wide.at[z, x, c], b_send.at[step - 1], b_recv.at[step - 1], to)
        remote(hid, held.at[x, c], h_send.at[step - 1], h_recv.at[step - 1], to)

    rounds = nz // 2

    def ring_block(s, side, halved):
        away = nz - s if side == 0 else s
        from_z = lax.rem(z + away, nz)
        if halved:
            return wide.at[from_z, pl.ds(side * (nx // 2), nx // 2), c]
        return wide.at[from_z, :, c]

    def ring_sent(s, side):
        return ring_block(s, side, s == rounds - 1)

    def ring(s):
        if s == 0:
            for step in range(1, nx):
                drained(rmap, b_recv.at[step - 1])
            remote(wide.at[z, :, c], wide.at[z, :, c], s_send, s_recv, other)
        else:
            for side in range(2):
                some = ring_block(s, side, s == rounds)
                drained(some, z_recv.at[side, s - 1])
                remote(some, some, s_send, s_recv, other)
        if s < rounds:
            for side in range(2):
                to = (lax.rem(z + (1 if side == 0 else nz - 1), nz), x, c, y)
                some = ring_sent(s, side)
                remote(some, some, z_send.at[side, s], z_recv.at[side, s], to)

    blocks, span = rtile.shape[0], rtile.shape[1]
    row = lax.broadcasted_iota(jnp.int32, (toks, 128), 0)
    reach = [1 << s for s in range(toks.bit_length() - 1)]

    def gates():
        for b in range(blocks):
            here = pl.ds(b * span, span)
            some = xmem[:, here]
            rec = jax.nn.sigmoid(jnp.dot(some, rtile[b], preferred_element_type=F32))
            inp = jax.nn.sigmoid(jnp.dot(some, itile[b], preferred_element_type=F32))
            speed = -8.0 * fade[:, here]
            log_decay = rec * speed + extra[...]
            decay = jnp.exp(log_decay)
            spare = 1.0 - jnp.exp(2.0 * log_decay)
            scale = jnp.sqrt(jnp.maximum(spare, 0.01))
            gated = inp * some.astype(F32)
            slope = jnp.where(spare > 0.01, -decay * decay / scale, 0.0)
            level = hid[:, here].astype(F32) - scale * gated + slope * gated
            pieces[0, :, here] = level * speed * rec * (1.0 - rec)
            pieces[1, :, here] = scale * gated * (1.0 - inp)
            pieces[2, :, here] = scale * inp
            pieces[4, :, here] = decay

    def tell(src, dst, send, recv):
        def one(i, _):
            remote(src, dst.at[index], send, recv, sp_at(i))
            return 0

        lax.fori_loop(1, plane, one, 0)

    def products():
        for i in range(width // 128):
            here = pl.ds(i * 128, 128)
            decay = pieces[4, :, here]
            prod = jnp.where(row < toks - 1, pltpu.roll(decay, toks - 1, 0), 1.0)
            for n, s in enumerate(reach):
                inside = row < toks - s
                levels[n, :, here] = jnp.where(inside, prod, 0.0)
                prod = prod * jnp.where(inside, pltpu.roll(prod, toks - s, 0), 1.0)
            pieces[3, :, here] = prod
            small[0, pl.ds(i, 1), :] = decay[0:1] * prod[0:1]
        betas[index] = small[0]
        tell(small.at[0], betas, a_send.at[0], a_recv.at[0])

    def weigh_all():
        drained(betas.at[pl.ds(0, plane - 1)], a_recv.at[0])

        def weigh(j, run):
            later = j > index
            weights[j] = jnp.where(later, run, 0.0)
            return jnp.where(later, run * betas[j], 1.0)

        lax.fori_loop(0, plane, weigh, jnp.ones((width // 128, 128), F32))

    def block(k, turn):
        start = pl.multiple_of(c * half + k * group, cap)
        return xy.at[:, pl.ds(start, group), cols(turn)]

    def across(k, turn):
        remote(block(k, turn), block(k, turn), c_send, c_recv, other)

    def along(k, turn, to, send, recv):
        remote(block(k, turn), block(k, turn), send, recv, to)

    turn_dims = (((1,), (1,)), ((), ()))
    piece = min(256, half)

    def forward(side, turn, first):
        def some(i, _):
            m, n = i // (half // piece), lax.rem(i, half // piece)
            here = pl.ds(pl.multiple_of(side * half + n * piece, cap), piece)
            got = lax.dot_general(
                wts[m, :, cols(turn)], xy[m // 2, here, cols(turn)], turn_dims,
                preferred_element_type=F32,
            )
            if first:
                accs[m, :, here] = got
            else:
                accs[m, :, here] += got
            return 0

        lax.fori_loop(0, 3 * (half // piece), some, 0)

    for turn in range(nz + 3):
        k = turn
        if k < nz:
            if k == 0:
                drained(slots.at[:, pl.ds(0, group - cap), :], d_recv.at[0])
            else:
                drained(block(k, 0), d_recv.at[k])
            along(k, 0, up, y_send.at[0, k], y_recv.at[0, k])
            along(k, 0, down, y_send.at[1, k], y_recv.at[1, k])
            across(k, 0)
        k = turn - 2
        if 0 <= k < nz:
            drained(block(k, 3), y_recv.at[0, k])
            if k % 2 == 0:
                along(k, 3, up, f_send.at[k], f_recv.at[k])
            across(k, 3)
            drained(block(k, 1), y_recv.at[1, k])
            if k % 2 == 1:
                along(k, 1, down, f_send.at[k], f_recv.at[k])
            across(k, 1)
        if turn == nz + 2:
            forward(c, 3, False)
            forward(c, 1, False)
        k = turn - 3
        if 0 <= k < nz:
            drained(block(k, 2), f_recv.at[k])
            across(k, 2)
        if turn == nz // 2:
            gates()
        if turn == nz // 2 + 1:
            products()
        if turn == nz:
            for load in loads:
                load.wait()
            forward(c, 0, True)
            ring(0)
            for step in range(1, nx):
                drained(hid, h_recv.at[step - 1])
            remote(held.at[:, c], held.at[:, c], t_send, t_recv, other)
        if turn == nz + 2:
            ring(1)
    forward(c, 2, False)
    drained(xy.at[:, pl.ds(pl.multiple_of((1 - c) * half, cap), half), :], c_recv)
    for turn in range(4):
        forward(1 - c, turn, turn == 0)

    units = accs.shape[1]

    def activate(i, _):
        here = pl.ds(pl.multiple_of(i * 16, 16), 16)
        gate, wider, backed = accs[0, here, :], accs[1, here, :], accs[2, here, :]
        sig = jax.nn.sigmoid(gate)
        active = gate * sig
        acts[0, here, :] = (backed * wider * (sig * (1.0 + gate * (1.0 - sig)))).astype(BF16)
        acts[1, here, :] = (backed * active).astype(BF16)
        acts[2, here, :] = (active * wider).astype(BF16)
        return 0

    lax.fori_loop(0, units // 16, activate, 0)

    chunk = 2 * group
    chunks = nz // 2

    def step_rows(i):
        at = (chunks - 1 - i) * chunk
        lines = [
            pl.ds(pl.multiple_of(side * half + at, chunk), chunk) for side in (1 - c, c)
        ]
        left = [
            jnp.concatenate([jnp.transpose(acts[m, :, n]) for n in lines], axis=0)
            for m in range(2)
        ]

        def some(n, _):
            here = pl.ds(pl.multiple_of(n * width, 128), width)
            got = jnp.dot(left[0], wts[0, :, here], preferred_element_type=F32)
            got = got + jnp.dot(left[1], wts[1, :, here], preferred_element_type=F32)
            give_rows[pl.ds(at, chunk), here] = got[:chunk].astype(BF16)
            own_rows[pl.ds(at, chunk), here] = got[chunk:].astype(BF16)
            return 0

        lax.fori_loop(0, ny, some, 0)
        span_of = pl.ds(at, chunk)
        remote(give_rows.at[span_of], pair.at[span_of], p_send.at[i], p_recv.at[i], other)

    def step_pair(i):
        at = (chunks - 1 - i) * chunk
        span_of = pl.ds(at, chunk)
        drained(pair.at[span_of], p_recv.at[i])
        for turn in (2, 1, 3, 0):
            total = own_rows[span_of, cols(turn)].astype(F32)
            total = total + pair[span_of, cols(turn)].astype(F32)
            sums[turn, span_of, :] = total.astype(BF16)
        low, high = pl.ds(at, group), pl.ds(at + group, group)
        remote(sums.at[2, low], far.at[0, i], e_send.at[0, i], e_recv.at[0, i], up)
        remote(sums.at[2, high], far.at[1, i], e_send.at[1, i], e_recv.at[1, i], down)
        remote(sums.at[1, high], near.at[0, high], e_send.at[2, i], e_recv.at[2, i], up)
        remote(sums.at[3, low], near.at[1, low], e_send.at[3, i], e_recv.at[3, i], down)

    def step_far(i):
        at = (chunks - 1 - i) * chunk
        low, high = pl.ds(at, group), pl.ds(at + group, group)
        for side, turn, where, to in ((0, 1, low, up), (1, 3, high, down)):
            drained(far.at[side, i], e_recv.at[side, i])
            total = sums[turn, where, :].astype(F32) + far[side, i].astype(F32)
            sums[turn, where, :] = total.astype(BF16)
            remote(
                sums.at[turn, where], near.at[side, where], e_send.at[4 + side, i],
                e_recv.at[4 + side, i], to,
            )

    def give(i, _):
        k, sx = i // nx, lax.rem(x + lax.rem(i, nx), nx)
        to = (lax.rem(z + nz - offset_of(k, nz), nz), sx, c, y)
        remote(
            mine.at[pl.ds(pl.multiple_of((k * nx + sx) * cap, cap), cap), :],
            back.at[mine_too, :],
            r_send, r_recv, to,
        )
        return 0

    def step_near(i):
        at = (chunks - 1 - i) * chunk
        span_of = pl.ds(at, chunk)
        for n in range(2, 6):
            drained(far.at[0, i], e_recv.at[n, i])
        total = sums[0, span_of, :].astype(F32) + near[0, span_of, :].astype(F32)
        mine[span_of, :] = (total + near[1, span_of, :].astype(F32)).astype(BF16)
        k = (chunks - 1 - i) * 2
        if k == 0:
            back[mine_too, :] = mine[pl.ds(pl.multiple_of(x * cap, cap), cap), :]
        lax.fori_loop(max(k * nx, 1), (k + 2) * nx, give, 0)

    tall = 256

    def weight_grad(m):
        def some(i, _):
            here = pl.ds(pl.multiple_of(i * tall, tall), tall)
            grads[m, :, here] = jnp.dot(
                acts[m], xy[m // 2, :, here], preferred_element_type=F32
            ).astype(BF16)
            return 0

        lax.fori_loop(0, feats // tall, some, 0)
        pltpu.make_async_copy(grads.at[m], outs[m], out_sem.at[m]).start()

    later_rings = list(range(2, rounds + 1))
    step_rows(0)
    for i in range(1, chunks):
        step_rows(i)
        step_pair(i - 1)
    step_pair(chunks - 1)
    todo = 0
    for i in range(chunks):
        step_far(i)
        if later_rings:
            ring(later_rings.pop(0))
        if i >= 1:
            if todo < 3:
                weight_grad(todo)
                todo += 1
            step_near(i - 1)
    while todo < 3:
        weight_grad(todo)
        todo += 1
    step_near(chunks - 1)
    for s in later_rings:
        ring(s)
    weigh_all()

    slot = lax.broadcasted_iota(jnp.int32, (toks, half), 1)
    chosen = (slot == spots[:, 0:1]) | (slot == spots[:, 1:2])
    onehot = jnp.where(chosen, 1.0, 0.0).astype(BF16)
    drained(back.at[pl.ds(0, half - cap), :], r_recv)
    moe[:, cols(0)] = jnp.dot(onehot, back[...], preferred_element_type=F32).astype(BF16)
    for step in (1, 3, 2):
        remote(
            moe.at[:, cols(0)], moe.at[:, cols(0)], m_send.at[step - 1], m_recv.at[step - 1],
            (z, x, c, lax.rem(y + step, ny)),
        )
    drained(wide.at[:, :, 1 - c], s_recv)
    drained(held.at[:, 1 - c], t_recv)
    for step in (1, 3, 2):
        drained(moe.at[:, cols(ny - step)], m_recv.at[step - 1])
    mixed[...] = (cot[...].astype(F32) + moe[...].astype(F32)).astype(BF16)

    lines = rmap.shape[0]
    turned[...] = jnp.transpose(mixed[...]).reshape(nz, 2 * nx, lines, toks)
    spot = x * 2 + c
    ours = pl.ds(pl.multiple_of(spot * toks, toks), toks)
    cross[:, :, ours] = turned[:, spot]
    for step in range(1, 2 * nx):
        to = lax.rem(spot + step, 2 * nx)
        remote(
            turned.at[:, to], cross.at[:, :, ours], g_send.at[step - 1], g_recv.at[step - 1],
            (z, to // 2, lax.rem(to, 2), y),
        )

    state = jnp.dot(mixed[...], wide[...].reshape(-1, width), preferred_element_type=F32)
    for n, s in enumerate(reach):
        state = state + levels[n] * pltpu.roll(state, toks - s, 0)
    first = pieces[4, 0:1, :] * state[0:1]
    for i in range(width // 128):
        small[1, pl.ds(i, 1), :] = first[:, i * 128 : (i + 1) * 128]
    alphas[index] = small[1]
    tell(small.at[1], alphas, a_send.at[1], a_recv.at[1])

    for step in range(1, 2 * nx):
        drained(turned.at[:, 0], g_recv.at[step - 1])
    total = jnp.dot(
        cross[...].reshape(nz * lines, 2 * nx * toks),
        held[...].reshape(2 * nx * toks, width),
        preferred_element_type=F32,
    )
    fold[...] = total.astype(BF16).reshape(nz, lines, width)
    rest[z] = fold[z]
    for step in range(1, nz):
        to = lax.rem(z + step, nz)
        remote(fold.at[to], rest.at[z], q_send.at[step - 1], q_recv.at[step - 1], (to, x, c, y))

    drained(alphas.at[pl.ds(0, plane - 1)], a_recv.at[1])
    carried = jnp.sum(weights[...] * alphas[...], axis=0)
    carried = jnp.concatenate([carried[i : i + 1] for i in range(width // 128)], axis=1)
    state = state + pieces[3] * carried
    grad_rec = (state * pieces[0]).astype(BF16)
    grad_in = (state * pieces[1]).astype(BF16)
    direct = state * pieces[2]
    for b in range(blocks):
        here = slice(b * span, (b + 1) * span)
        lru_out[:, here] = (
            direct[:, here]
            + lax.dot_general(grad_rec[:, here], rtile[b], turn_dims, preferred_element_type=F32)
            + lax.dot_general(grad_in[:, here], itile[b], turn_dims, preferred_element_type=F32)
        )

    for step in range(1, nz):
        drained(fold.at[0], q_recv.at[step - 1])
    summed = rest[0].astype(F32)
    for i in range(1, nz):
        summed = summed + rest[i].astype(F32)
    proj_out[...] = summed

    whole = xy.at[:, pl.ds(pl.multiple_of(c * half, cap), half), :]
    drained(whole, c_send)
    drained(slots.at[:, pl.ds(0, half - cap), :], d_send)
    for k in range(nz):
        drained(block(k, 0), y_send.at[0, k])
        drained(block(k, 0), y_send.at[1, k])
        drained(block(k, 2), f_send.at[k])
    for i in range(chunks):
        drained(pair.at[pl.ds(0, chunk)], p_send.at[i])
        for n in range(6):
            drained(far.at[0, 0], e_send.at[n, i])
    drained(back.at[pl.ds(0, half - cap), :], r_send)
    for step in (1, 2, 3):
        drained(moe.at[:, cols(0)], m_send.at[step - 1])
    for step in range(nx - 1):
        drained(rmap, b_send.at[step])
        drained(hid, h_send.at[step])
    for s in range(rounds):
        for side in range(2):
            drained(ring_sent(s, side), z_send.at[side, s])
    drained(wide.at[:, :, c], s_send)
    drained(held.at[:, c], t_send)
    for i in range(2):
        drained(betas.at[pl.ds(0, plane - 1)], a_send.at[i])
    for step in range(2 * nx - 1):
        drained(turned.at[:, 0], g_send.at[step])
    for step in range(nz - 1):
        drained(fold.at[0], q_send.at[step])
    for m in range(3):
        pltpu.make_async_copy(grads.at[m], outs[m], out_sem.at[m]).wait()


def layer_entry(dims, cap, *refs):
    layer_kernel(dims, cap, *refs[:12], refs[12:15], refs[15:18], *refs[18:])


def layer(dims, cap, *operands):
    target, spots, share, cot, rows, rmap, xmem, hid, fade, extra, rtile, itile, *maps = operands
    nz, nx, ny = dims
    toks, feats = cot.shape
    half, width, group = nz * nx * cap, feats // ny, nx * cap
    lines, units = rmap.shape[0], maps[0].shape[0]
    plane, lanes, steps = nz * nx * 2, width // 128, toks.bit_length() - 1
    vmem, anyw = pl.BlockSpec(memory_space=pltpu.VMEM), pl.BlockSpec(memory_space=pl.ANY)
    dma = pltpu.SemaphoreType.DMA
    return pl.pallas_call(
        functools.partial(layer_entry, dims, cap),
        out_shape=[jax.ShapeDtypeStruct((units, feats), BF16)] * 3
        + [
            jax.ShapeDtypeStruct((lines, width), F32),
            jax.ShapeDtypeStruct((toks, width), F32),
        ],
        in_specs=[vmem] * 12 + [anyw] * 3,
        out_specs=[anyw] * 3 + [vmem] * 2,
        scratch_shapes=[
            pltpu.VMEM((2, half, width), BF16),
            pltpu.VMEM((2, 2 * half, feats), BF16),
            pltpu.VMEM((3, units, feats), BF16),
            pltpu.VMEM((3, units, 2 * half), F32),
            pltpu.VMEM((3, units, 2 * half), BF16),
            pltpu.VMEM((half, feats), BF16),
            pltpu.VMEM((half, feats), BF16),
            pltpu.VMEM((half, feats), BF16),
            pltpu.VMEM((4, half, width), BF16),
            pltpu.VMEM((2, nz // 2, group, width), BF16),
            pltpu.VMEM((2, half, width), BF16),
            pltpu.VMEM((half, width), BF16),
            pltpu.VMEM((half, width), BF16),
            pltpu.VMEM((toks, feats), BF16),
            pltpu.VMEM((toks, feats), BF16),
            pltpu.VMEM((3, units, feats), BF16),
            pltpu.VMEM((nz, nx, 2, lines, width), BF16),
            pltpu.VMEM((nx, 2, toks, width), BF16),
            pltpu.VMEM((nz, 2 * nx, lines, toks), BF16),
            pltpu.VMEM((nz, lines, 2 * nx * toks), BF16),
            pltpu.VMEM((nz, lines, width), BF16),
            pltpu.VMEM((nz, lines, width), BF16),
            pltpu.VMEM((steps, toks, width), F32),
            pltpu.VMEM((5, toks, width), F32),
            pltpu.VMEM((plane, lanes, 128), F32),
            pltpu.VMEM((plane, lanes, 128), F32),
            pltpu.VMEM((plane, lanes, 128), F32),
            pltpu.VMEM((2, lanes, 128), F32),
            dma, dma((3,)), dma((3,)),
            dma, dma((nz,)), dma((2, nz)), dma((2, nz)), dma((nz,)), dma((nz,)), dma, dma,
            dma((nz // 2,)), dma((nz // 2,)), dma((6, nz // 2)), dma((6, nz // 2)), dma, dma,
            dma((3,)), dma((3,)), dma((nx - 1,)), dma((nx - 1,)), dma((2, nz // 2)),
            dma((2, nz // 2)), dma, dma, dma((nx - 1,)), dma((nx - 1,)), dma, dma, dma((2,)),
            dma((2,)), dma((2 * nx - 1,)), dma((2 * nx - 1,)), dma((nz - 1,)), dma((nz - 1,)),
        ],
        compiler_params=pltpu.CompilerParams(
            collective_id=0, has_side_effects=True, vmem_limit_bytes=60 * 2**20
        ),
        name="layer",
    )(*operands)


def local(
    result_cotangent_values,
    specialist_entry_vectors,
    chosen_specialists,
    specialist_mixing_shares,
    specialist_switch_maps,
    specialist_widen_maps,
    specialist_shrink_maps,
    memory_readout_map,
    memory_source_vectors,
    memory_hidden_values,
    feature_fading_speed,
    extra_log_fading,
    memory_switch_tiles,
    entry_switch_tiles,
):
    tok_rows, feature_count = result_cotangent_values.shape
    route_count = chosen_specialists.shape[1]
    sp_count = lax.axis_size(SP)
    expert_count = sp_count // SLICES
    capacity = min(tok_rows, 4 * tok_rows // expert_count)
    pairs = chosen_specialists.T.reshape(-1)
    order = (jnp.arange(tok_rows)[None, :] * route_count + jnp.arange(route_count)[:, None]).reshape(-1)
    earlier = (pairs[:, None] == pairs[None, :]) & (order[:, None] < order[None, :])
    target = pairs * capacity + jnp.sum(earlier.astype(jnp.int32), axis=0)
    dims = (lax.axis_size("sp_0"), lax.axis_size("sp_1"), lax.axis_size("tp"))
    gate_weight_grad, up_weight_grad, down_grad, out_proj_grad, lru_input_grad = layer(
        dims,
        capacity,
        target[None, :],
        target.reshape(route_count, tok_rows).T,
        specialist_mixing_shares,
        result_cotangent_values,
        specialist_entry_vectors,
        memory_readout_map,
        memory_source_vectors,
        memory_hidden_values,
        feature_fading_speed[None, :],
        extra_log_fading[:, None],
        memory_switch_tiles,
        entry_switch_tiles,
        specialist_switch_maps[0].T,
        specialist_widen_maps[0].T,
        specialist_shrink_maps[0],
    )
    return (
        gate_weight_grad.T[None],
        up_weight_grad.T[None],
        down_grad[None],
        out_proj_grad,
        lru_input_grad,
    )


def solution(mesh):
    finer = Mesh(mesh.devices.reshape(8, 4, 2, mesh.shape["tp"]), ("sp_0", "sp_1", "sp_2", "tp"))
    in_specs = (
        P(SP, None),
        P(SP, None),
        P(SP, None),
        P(SP, None),
        P(SP, None, "tp"),
        P(SP, None, "tp"),
        P(SP, "tp", None),
        P(SP, "tp"),
        P(SP, "tp"),
        P(SP, "tp"),
        P("tp"),
        P(SP),
        P("tp", None, None),
        P("tp", None, None),
    )
    out_specs = (P(SP, None, "tp"), P(SP, None, "tp"), P(SP, "tp", None), P(SP, "tp"), P(SP, "tp"))
    return jax.shard_map(local, mesh=finer, in_specs=in_specs, out_specs=out_specs, check_vma=False)
```

```python
import functools

import jax
import jax.numpy as jnp
from jax import lax
from jax.experimental import pallas as pl
from jax.experimental.pallas import tpu as pltpu
from jax.sharding import Mesh
from jax.sharding import PartitionSpec as P

SLICES = 2
SP = ("sp_0", "sp_1", "sp_2")
MESH = pl.DeviceIdType.MESH
F32, BF16 = jnp.float32, jnp.bfloat16


def place():
    return tuple(lax.axis_index(n) for n in ("sp_0", "sp_1", "sp_2", "tp"))


def offset_of(k, count):
    odd = lax.rem(k, 2)
    return lax.rem(odd * ((k + 1) // 2) + (1 - odd) * (count - k // 2), count)


def drained(ref, sem):
    pltpu.make_async_copy(ref, ref, sem).wait()


def layer_kernel(
    dims, cap, chosen, share, cot, rows, rmap, xmem, hid, fade, extra, rtile, itile, maps,
    outs, proj_out, lru_out,
    slots, xy, wts, flipped, accs, acts, across_acts, give_rows, own_rows, pair, sums, far, near, back, mine, moe, mixed,
    wide, held, turned, cross, fold, rest, levels, pieces, alphas, betas, weights, small, picked,
    in_sem, out_sem, d_send, d_recv, y_send, y_recv, f_send, f_recv, c_send, c_recv,
    p_send, p_recv, e_send, e_recv, r_send, r_recv, m_send, m_recv, b_send, b_recv, z_send, z_recv,
    s_send, s_recv, h_send, h_recv, t_send, t_recv, a_send, a_recv, g_send, g_recv, q_send, q_recv,
):
    nz, nx, ny = dims
    z, x, c, y = place()
    plane = nz * nx * 2
    index = (z * nx + x) * 2 + c
    me = z * nx + x
    toks, feats = cot.shape
    width = feats // ny
    half = nz * nx * cap
    group = nx * cap
    other = (z, x, 1 - c, y)
    up, down = (z, x, c, lax.rem(y + 1, ny)), (z, x, c, lax.rem(y + 3, ny))
    barrier = pltpu.get_barrier_semaphore()

    def sp_at(i):
        i = lax.rem(index + i, plane)
        return (i // (2 * nx), lax.rem(i // 2, nx), lax.rem(i, 2), y)

    def greet(i, _):
        pl.semaphore_signal(barrier, inc=1, device_id=sp_at(i), device_id_type=MESH)
        return 0

    lax.fori_loop(1, plane, greet, 0)
    for step in (1, 2, 3):
        to = (z, x, c, lax.rem(y + step, ny))
        pl.semaphore_signal(barrier, inc=1, device_id=to, device_id_type=MESH)

    def cols(turn):
        return pl.ds(pl.multiple_of(lax.rem(y + turn, ny) * width, 128), width)

    def remote(src, dst, send, recv, to):
        pltpu.make_async_remote_copy(
            src_ref=src, dst_ref=dst, send_sem=send, recv_sem=recv, device_id=to,
            device_id_type=MESH,
        ).start()

    loads = [pltpu.make_async_copy(maps[m], wts.at[m], in_sem.at[m]) for m in range(3)]
    for load in loads:
        load.start()
    wide[z, x, c] = rmap[...]
    held[x, c] = hid[...]

    def upright(line):
        return jnp.transpose(jnp.broadcast_to(line, (toks, toks)))

    experts = [chosen[k : k + 1, :].astype(F32) for k in range(2)]
    earlier = [
        lax.broadcasted_iota(jnp.int32, (toks, toks), 0)
        < lax.broadcasted_iota(jnp.int32, (toks, toks), 1) + k
        for k in range(2)
    ]
    places = []
    for k in range(2):
        rank = jnp.zeros((1, toks), F32)
        for j in range(2):
            same = (upright(experts[j]) == experts[k]) & earlier[1 if j < k else 0]
            rank = rank + jnp.sum(jnp.where(same, 1.0, 0.0), axis=0, keepdims=True)
        places.append(experts[k] * cap + rank)
    slot = lax.broadcasted_iota(jnp.int32, (half, 2 * toks), 0).astype(F32)
    onehot = jnp.where(slot == jnp.concatenate(places, axis=1), 1.0, 0.0).astype(BF16)
    some = rows[:, cols(0)]
    slots[0] = jnp.dot(
        onehot, jnp.concatenate([some, some], axis=0), preferred_element_type=F32
    ).astype(BF16)
    some = cot[:, cols(0)].astype(F32)
    scaled = [(upright(share[k : k + 1, :])[:, 0:1] * some).astype(BF16) for k in range(2)]
    slots[1] = jnp.dot(
        onehot, jnp.concatenate(scaled, axis=0), preferred_element_type=F32
    ).astype(BF16)
    slot = lax.broadcasted_iota(jnp.int32, (toks, half), 1).astype(F32)
    found = [slot == upright(places[k])[:, 0:1] for k in range(2)]
    picked[...] = jnp.where(found[0] | found[1], 1.0, 0.0).astype(BF16)

    def source(e):
        return slots.at[:, pl.ds(pl.multiple_of(e * cap, cap), cap), :]

    def landing(k):
        start = pl.multiple_of(c * half + (k * nx + x) * cap, cap)
        return xy.at[:, pl.ds(start, cap), cols(0)]

    here = pl.ds(pl.multiple_of(c * half + x * cap, cap), cap)
    mine_too = pl.ds(pl.multiple_of(me * cap, cap), cap)
    for i in range(2):
        xy[i, here, cols(0)] = slots[i, mine_too, :]
    pl.semaphore_wait(barrier, plane - 1 + 3)

    def push(k):
        def one(dx, _):
            tz, tx = lax.rem(z + offset_of(k, nz), nz), lax.rem(x + dx, nx)
            remote(source(tz * nx + tx), landing(k), d_send, d_recv.at[k], (tz, tx, c, y))
            return 0

        lax.fori_loop(1 if k == 0 else 0, nx, one, 0)

    ahead = 3
    for k in range(ahead):
        push(k)

    def push_rest():
        for step in range(1, nx):
            to = (z, lax.rem(x + step, nx), c, y)
            remote(rmap, wide.at[z, x, c], b_send.at[step - 1], b_recv.at[step - 1], to)
            remote(hid, held.at[x, c], h_send.at[step - 1], h_recv.at[step - 1], to)

    def hand_over():
        for step in range(1, nx):
            drained(hid, h_recv.at[step - 1])
        remote(held.at[:, c], held.at[:, c], t_send, t_recv, other)

    rounds = nz // 2

    def ring_block(s, side, halved):
        away = nz - s if side == 0 else s
        from_z = lax.rem(z + away, nz)
        if halved:
            return wide.at[from_z, pl.ds(side * (nx // 2), nx // 2), c]
        return wide.at[from_z, :, c]

    def ring_sent(s, side):
        return ring_block(s, side, s == rounds - 1)

    def ring(s):
        if s == 0:
            for step in range(1, nx):
                drained(rmap, b_recv.at[step - 1])
            remote(wide.at[z, :, c], wide.at[z, :, c], s_send, s_recv, other)
        else:
            for side in range(2):
                some = ring_block(s, side, s == rounds)
                drained(some, z_recv.at[side, s - 1])
                remote(some, some, s_send, s_recv, other)
        if s < rounds:
            for side in range(2):
                to = (lax.rem(z + (1 if side == 0 else nz - 1), nz), x, c, y)
                some = ring_sent(s, side)
                remote(some, some, z_send.at[side, s], z_recv.at[side, s], to)

    blocks, span = rtile.shape[0], rtile.shape[1]
    row = lax.broadcasted_iota(jnp.int32, (toks, 128), 0)
    reach = [1 << s for s in range(toks.bit_length() - 1)]

    def gates():
        for b in range(blocks):
            here = pl.ds(b * span, span)
            some = xmem[:, here]
            rec = jax.nn.sigmoid(jnp.dot(some, rtile[b], preferred_element_type=F32))
            inp = jax.nn.sigmoid(jnp.dot(some, itile[b], preferred_element_type=F32))
            speed = -8.0 * fade[:, here]
            log_decay = rec * speed + upright(extra[...])[:, 0:1]
            decay = jnp.exp(log_decay)
            spare = 1.0 - jnp.exp(2.0 * log_decay)
            scale = jnp.sqrt(jnp.maximum(spare, 0.01))
            gated = inp * some.astype(F32)
            slope = jnp.where(spare > 0.01, -decay * decay / scale, 0.0)
            level = hid[:, here].astype(F32) - scale * gated + slope * gated
            pieces[0, :, here] = level * speed * rec * (1.0 - rec)
            pieces[1, :, here] = scale * gated * (1.0 - inp)
            pieces[2, :, here] = scale * inp
            pieces[4, :, here] = decay

    def tell(src, dst, send, recv):
        def one(i, _):
            remote(src, dst.at[index], send, recv, sp_at(i))
            return 0

        lax.fori_loop(1, plane, one, 0)

    def products():
        for i in range(width // 128):
            here = pl.ds(i * 128, 128)
            decay = pieces[4, :, here]
            prod = jnp.where(row < toks - 1, pltpu.roll(decay, toks - 1, 0), 1.0)
            for n, s in enumerate(reach):
                inside = row < toks - s
                levels[n, :, here] = jnp.where(inside, prod, 0.0)
                prod = prod * jnp.where(inside, pltpu.roll(prod, toks - s, 0), 1.0)
            pieces[3, :, here] = prod
            small[0, pl.ds(i, 1), :] = decay[0:1] * prod[0:1]
        betas[index] = small[0]
        tell(small.at[0], betas, a_send.at[0], a_recv.at[0])

    def weigh_all():
        drained(betas.at[pl.ds(0, plane - 1)], a_recv.at[0])

        def weigh(j, run):
            later = j > index
            weights[j] = jnp.where(later, run, 0.0)
            return jnp.where(later, run * betas[j], 1.0)

        lax.fori_loop(0, plane, weigh, jnp.ones((width // 128, 128), F32))

    def block(k, turn):
        start = pl.multiple_of(c * half + k * group, cap)
        return xy.at[:, pl.ds(start, group), cols(turn)]

    def across(k, turn):
        remote(block(k, turn), block(k, turn), c_send, c_recv.at[k // (nz // 2), turn], other)

    def along(k, turn, to, send, recv):
        remote(block(k, turn), block(k, turn), send, recv, to)

    turn_dims = (((1,), (1,)), ((), ()))
    piece = half // 2
    units = accs.shape[2]

    def flip(m):
        loads[m].wait()

        def some(i, _):
            here = pl.ds(pl.multiple_of(i * 128, 128), 128)
            flipped[m, here, :] = jnp.transpose(wts[m, :, here])
            return 0

        lax.fori_loop(0, feats // 128, some, 0)

    def forward(own, part, turn):
        side = c if own else 1 - c
        here = pl.ds(pl.multiple_of(side * half + part * piece, cap), piece)
        if not own:
            drained(xy.at[:, here, cols(turn)], c_recv.at[part, turn])

        def some(m, _):
            got = jnp.dot(
                xy[m // 2, here, cols(turn)], flipped[m, cols(turn), :], preferred_element_type=F32
            )
            if turn == 0:
                accs[m, here, :] = got
            else:
                accs[m, here, :] += got
            return 0

        lax.fori_loop(0, 3, some, 0)

    def activate(part):
        tile = 16

        def some(i, _):
            side, n = i // (piece // tile), lax.rem(i, piece // tile)
            here = pl.ds(pl.multiple_of(side * half + part * piece + n * tile, tile), tile)
            gate, wider, backed = accs[0, here, :], accs[1, here, :], accs[2, here, :]
            sig = jax.nn.sigmoid(gate)
            active = gate * sig
            acts[0, here, :] = (backed * wider * (sig * (1.0 + gate * (1.0 - sig)))).astype(BF16)
            acts[1, here, :] = (backed * active).astype(BF16)
            acts[2, here, :] = (active * wider).astype(BF16)
            return 0

        lax.fori_loop(0, 2 * (piece // tile), some, 0)

    chunk = 2 * group
    chunks = nz // 2

    def step_rows(i):
        at = i * chunk
        lines = [
            pl.ds(pl.multiple_of(side * half + at, chunk), chunk) for side in (1 - c, c)
        ]
        left = [jnp.concatenate([acts[m, n, :] for n in lines], axis=0) for m in range(2)]

        def some(n, _):
            here = pl.ds(pl.multiple_of(n * width, 128), width)
            got = jnp.dot(left[0], wts[0, :, here], preferred_element_type=F32)
            got = got + jnp.dot(left[1], wts[1, :, here], preferred_element_type=F32)
            give_rows[pl.ds(at, chunk), here] = got[:chunk].astype(BF16)
            own_rows[pl.ds(at, chunk), here] = got[chunk:].astype(BF16)
            return 0

        lax.fori_loop(0, ny, some, 0)
        span_of = pl.ds(at, chunk)
        remote(give_rows.at[span_of], pair.at[span_of], p_send.at[i], p_recv.at[i], other)

    def step_pair(i):
        at = i * chunk
        span_of = pl.ds(at, chunk)
        drained(pair.at[span_of], p_recv.at[i])
        for turn in (2, 1, 3, 0):
            total = own_rows[span_of, cols(turn)].astype(F32)
            total = total + pair[span_of, cols(turn)].astype(F32)
            sums[turn, span_of, :] = total.astype(BF16)
        low, high = pl.ds(at, group), pl.ds(at + group, group)
        remote(sums.at[2, low], far.at[0, i], e_send.at[0, i], e_recv.at[0, i], up)
        remote(sums.at[2, high], far.at[1, i], e_send.at[1, i], e_recv.at[1, i], down)
        remote(sums.at[1, high], near.at[0, high], e_send.at[2, i], e_recv.at[2, i], up)
        remote(sums.at[3, low], near.at[1, low], e_send.at[3, i], e_recv.at[3, i], down)

    def step_far(i):
        at = i * chunk
        low, high = pl.ds(at, group), pl.ds(at + group, group)
        for side, turn, where, to in ((0, 1, low, up), (1, 3, high, down)):
            drained(far.at[side, i], e_recv.at[side, i])
            total = sums[turn, where, :].astype(F32) + far[side, i].astype(F32)
            sums[turn, where, :] = total.astype(BF16)
            remote(
                sums.at[turn, where], near.at[side, where], e_send.at[4 + side, i],
                e_recv.at[4 + side, i], to,
            )

    def give(i, _):
        k, sx = i // nx, lax.rem(x + lax.rem(i, nx), nx)
        to = (lax.rem(z + nz - offset_of(k, nz), nz), sx, c, y)
        remote(
            mine.at[pl.ds(pl.multiple_of((k * nx + sx) * cap, cap), cap), :],
            back.at[mine_too, :],
            r_send, r_recv, to,
        )
        return 0

    def step_near(i):
        at = i * chunk
        span_of = pl.ds(at, chunk)
        for n in range(2, 6):
            drained(far.at[0, i], e_recv.at[n, i])
        total = sums[0, span_of, :].astype(F32) + near[0, span_of, :].astype(F32)
        mine[span_of, :] = (total + near[1, span_of, :].astype(F32)).astype(BF16)
        k = i * 2
        if k == 0:
            back[mine_too, :] = mine[pl.ds(pl.multiple_of(x * cap, cap), cap), :]
        lax.fori_loop(max(k * nx, 1), (k + 2) * nx, give, 0)

    tall = 256

    def weight_grad(m):
        def turn_over(i, _):
            here = pl.ds(pl.multiple_of(i * 128, 128), 128)
            across_acts[:, here] = jnp.transpose(acts[m, here, :])
            return 0

        lax.fori_loop(0, 2 * half // 128, turn_over, 0)

        def some(i, _):
            here = pl.ds(pl.multiple_of(i * tall, tall), tall)
            wts[m, :, here] = jnp.dot(
                across_acts[...], xy[m // 2, :, here], preferred_element_type=F32
            ).astype(BF16)
            return 0

        lax.fori_loop(0, feats // tall, some, 0)
        pltpu.make_async_copy(wts.at[m], outs[m], out_sem.at[m]).start()

    def receive(k):
        if k == 0:
            drained(slots.at[:, pl.ds(0, group - cap), :], d_recv.at[0])
        else:
            drained(block(k, 0), d_recv.at[k])
        along(k, 0, up, y_send.at[0, k], y_recv.at[0, k])
        along(k, 0, down, y_send.at[1, k], y_recv.at[1, k])
        across(k, 0)
        if k + ahead < nz:
            push(k + ahead)

    def receive_near(k):
        drained(block(k, 3), y_recv.at[0, k])
        if k % 2 == 0:
            along(k, 3, up, f_send.at[k], f_recv.at[k])
        across(k, 3)
        drained(block(k, 1), y_recv.at[1, k])
        if k % 2 == 1:
            along(k, 1, down, f_send.at[k], f_recv.at[k])
        across(k, 1)

    def receive_far(k):
        drained(block(k, 2), f_recv.at[k])
        across(k, 2)

    def work(what, *args):
        return functools.partial(what, *args)

    mid = nz // 2
    fillers = {}
    for at, jobs in (
        (0, [work(flip, 0), work(flip, 2)]),
        (1, [work(flip, 1), work(gates)]),
        (2, [work(products)]),
        (3, [work(push_rest)]),
        (mid, [work(forward, True, 0, 0)]),
        (mid + 1, [work(forward, False, 0, 0), work(forward, True, 0, 3)]),
        (mid + 2, [work(forward, True, 0, 1), work(forward, False, 0, 3)]),
        (mid + 3, [work(forward, True, 0, 2), work(forward, False, 0, 1)]),
        (nz, [work(forward, False, 0, 2), work(ring, 0), work(forward, True, 1, 0)]),
        (nz + 1, [work(activate, 0), work(hand_over), work(step_rows, 0),
                  work(forward, False, 1, 0), work(forward, True, 1, 3)]),
        (nz + 2, [work(step_rows, 1), work(forward, True, 1, 1), work(forward, False, 1, 3)]),
    ):
        fillers.setdefault(at, []).extend(jobs)
    for turn in range(nz + 3):
        if turn < nz:
            receive(turn)
        if 0 <= turn - 2 < nz:
            receive_near(turn - 2)
        if 0 <= turn - 3 < nz - 1:
            receive_far(turn - 3)
        for job in fillers.get(turn, []):
            job()
    receive_far(nz - 1)
    early = chunks // 2
    for i in range(early):
        step_pair(i)
    ring(1)
    forward(False, 1, 1)
    forward(True, 1, 2)
    forward(False, 1, 2)
    activate(1)
    later_rings = list(range(2, rounds + 1))
    for i in range(early):
        step_rows(early + i)
        step_far(i)
    for i in range(early):
        step_pair(early + i)
        step_near(i)
    if later_rings:
        ring(later_rings.pop(0))
    for i in range(early):
        step_far(early + i)
    for i in range(early):
        if later_rings:
            ring(later_rings.pop(0))
        step_near(early + i)
    weight_grad(0)
    for s in later_rings:
        ring(s)
    weigh_all()

    drained(back.at[pl.ds(0, half - cap), :], r_recv)
    moe[:, cols(0)] = jnp.dot(picked[...], back[...], preferred_element_type=F32).astype(BF16)
    for step in (1, 3, 2):
        remote(
            moe.at[:, cols(0)], moe.at[:, cols(0)], m_send.at[step - 1], m_recv.at[step - 1],
            (z, x, c, lax.rem(y + step, ny)),
        )
    weight_grad(1)
    drained(wide.at[:, :, 1 - c], s_recv)
    drained(held.at[:, 1 - c], t_recv)
    for step in (1, 3, 2):
        drained(moe.at[:, cols(ny - step)], m_recv.at[step - 1])
    mixed[...] = (cot[...].astype(F32) + moe[...].astype(F32)).astype(BF16)

    lines = rmap.shape[0]
    turned[...] = jnp.transpose(mixed[...]).reshape(nz, 2 * nx, lines, toks)
    spot = x * 2 + c
    ours = pl.ds(pl.multiple_of(spot * toks, toks), toks)
    cross[:, :, ours] = turned[:, spot]
    for step in range(1, 2 * nx):
        to = lax.rem(spot + step, 2 * nx)
        remote(
            turned.at[:, to], cross.at[:, :, ours], g_send.at[step - 1], g_recv.at[step - 1],
            (z, to // 2, lax.rem(to, 2), y),
        )

    state = jnp.dot(mixed[...], wide[...].reshape(-1, width), preferred_element_type=F32)
    for n, s in enumerate(reach):
        state = state + levels[n] * pltpu.roll(state, toks - s, 0)
    first = pieces[4, 0:1, :] * state[0:1]
    for i in range(width // 128):
        small[1, pl.ds(i, 1), :] = first[:, i * 128 : (i + 1) * 128]
    alphas[index] = small[1]
    tell(small.at[1], alphas, a_send.at[1], a_recv.at[1])

    for step in range(1, 2 * nx):
        drained(turned.at[:, 0], g_recv.at[step - 1])
    total = jnp.dot(
        cross[...].reshape(nz * lines, 2 * nx * toks),
        held[...].reshape(2 * nx * toks, width),
        preferred_element_type=F32,
    )
    fold[...] = total.astype(BF16).reshape(nz, lines, width)
    rest[z] = fold[z]
    for step in range(1, nz):
        to = lax.rem(z + step, nz)
        remote(fold.at[to], rest.at[z], q_send.at[step - 1], q_recv.at[step - 1], (to, x, c, y))

    drained(alphas.at[pl.ds(0, plane - 1)], a_recv.at[1])
    carried = jnp.sum(weights[...] * alphas[...], axis=0)
    carried = jnp.concatenate([carried[i : i + 1] for i in range(width // 128)], axis=1)
    state = state + pieces[3] * carried
    grad_rec = (state * pieces[0]).astype(BF16)
    grad_in = (state * pieces[1]).astype(BF16)
    direct = state * pieces[2]
    for b in range(blocks):
        here = slice(b * span, (b + 1) * span)
        lru_out[:, here] = (
            direct[:, here]
            + lax.dot_general(grad_rec[:, here], rtile[b], turn_dims, preferred_element_type=F32)
            + lax.dot_general(grad_in[:, here], itile[b], turn_dims, preferred_element_type=F32)
        )

    weight_grad(2)
    for step in range(1, nz):
        drained(fold.at[0], q_recv.at[step - 1])
    summed = rest[0].astype(F32)
    for i in range(1, nz):
        summed = summed + rest[i].astype(F32)
    proj_out[...] = summed

    whole = xy.at[:, pl.ds(pl.multiple_of(c * half, cap), half), :]
    drained(whole, c_send)
    drained(slots.at[:, pl.ds(0, half - cap), :], d_send)
    for k in range(nz):
        drained(block(k, 0), y_send.at[0, k])
        drained(block(k, 0), y_send.at[1, k])
        drained(block(k, 2), f_send.at[k])
    for i in range(chunks):
        drained(pair.at[pl.ds(0, chunk)], p_send.at[i])
        for n in range(6):
            drained(far.at[0, 0], e_send.at[n, i])
    drained(back.at[pl.ds(0, half - cap), :], r_send)
    for step in (1, 2, 3):
        drained(moe.at[:, cols(0)], m_send.at[step - 1])
    for step in range(nx - 1):
        drained(rmap, b_send.at[step])
        drained(hid, h_send.at[step])
    for s in range(rounds):
        for side in range(2):
            drained(ring_sent(s, side), z_send.at[side, s])
    drained(wide.at[:, :, c], s_send)
    drained(held.at[:, c], t_send)
    for i in range(2):
        drained(betas.at[pl.ds(0, plane - 1)], a_send.at[i])
    for step in range(2 * nx - 1):
        drained(turned.at[:, 0], g_send.at[step])
    for step in range(nz - 1):
        drained(fold.at[0], q_send.at[step])
    for m in range(3):
        pltpu.make_async_copy(wts.at[m], outs[m], out_sem.at[m]).wait()


def layer_entry(dims, cap, *refs):
    layer_kernel(dims, cap, *refs[:11], refs[11:14], refs[14:17], *refs[17:])


def layer(dims, cap, *operands):
    chosen, share, cot, rows, rmap, xmem, hid, fade, extra, rtile, itile, *maps = operands
    nz, nx, ny = dims
    toks, feats = cot.shape
    half, width, group = nz * nx * cap, feats // ny, nx * cap
    lines, units = rmap.shape[0], maps[0].shape[0]
    plane, lanes, steps = nz * nx * 2, width // 128, toks.bit_length() - 1
    vmem, anyw = pl.BlockSpec(memory_space=pltpu.VMEM), pl.BlockSpec(memory_space=pl.ANY)
    dma = pltpu.SemaphoreType.DMA
    return pl.pallas_call(
        functools.partial(layer_entry, dims, cap),
        out_shape=[jax.ShapeDtypeStruct((units, feats), BF16)] * 3
        + [
            jax.ShapeDtypeStruct((lines, width), F32),
            jax.ShapeDtypeStruct((toks, width), F32),
        ],
        in_specs=[vmem] * 11 + [anyw] * 3,
        out_specs=[anyw] * 3 + [vmem] * 2,
        scratch_shapes=[
            pltpu.VMEM((2, half, width), BF16),
            pltpu.VMEM((2, 2 * half, feats), BF16),
            pltpu.VMEM((3, units, feats), BF16),
            pltpu.VMEM((3, feats, units), BF16),
            pltpu.VMEM((3, 2 * half, units), F32),
            pltpu.VMEM((3, 2 * half, units), BF16),
            pltpu.VMEM((units, 2 * half), BF16),
            pltpu.VMEM((half, feats), BF16),
            pltpu.VMEM((half, feats), BF16),
            pltpu.VMEM((half, feats), BF16),
            pltpu.VMEM((4, half, width), BF16),
            pltpu.VMEM((2, nz // 2, group, width), BF16),
            pltpu.VMEM((2, half, width), BF16),
            pltpu.VMEM((half, width), BF16),
            pltpu.VMEM((half, width), BF16),
            pltpu.VMEM((toks, feats), BF16),
            pltpu.VMEM((toks, feats), BF16),
            pltpu.VMEM((nz, nx, 2, lines, width), BF16),
            pltpu.VMEM((nx, 2, toks, width), BF16),
            pltpu.VMEM((nz, 2 * nx, lines, toks), BF16),
            pltpu.VMEM((nz, lines, 2 * nx * toks), BF16),
            pltpu.VMEM((nz, lines, width), BF16),
            pltpu.VMEM((nz, lines, width), BF16),
            pltpu.VMEM((steps, toks, width), F32),
            pltpu.VMEM((5, toks, width), F32),
            pltpu.VMEM((plane, lanes, 128), F32),
            pltpu.VMEM((plane, lanes, 128), F32),
            pltpu.VMEM((plane, lanes, 128), F32),
            pltpu.VMEM((2, lanes, 128), F32),
            pltpu.VMEM((toks, half), BF16),
            dma((3,)), dma((3,)),
            dma, dma((nz,)), dma((2, nz)), dma((2, nz)), dma((nz,)), dma((nz,)), dma, dma((2, 4)),
            dma((nz // 2,)), dma((nz // 2,)), dma((6, nz // 2)), dma((6, nz // 2)), dma, dma,
            dma((3,)), dma((3,)), dma((nx - 1,)), dma((nx - 1,)), dma((2, nz // 2)),
            dma((2, nz // 2)), dma, dma, dma((nx - 1,)), dma((nx - 1,)), dma, dma, dma((2,)),
            dma((2,)), dma((2 * nx - 1,)), dma((2 * nx - 1,)), dma((nz - 1,)), dma((nz - 1,)),
        ],
        compiler_params=pltpu.CompilerParams(
            collective_id=0, has_side_effects=True, vmem_limit_bytes=60 * 2**20
        ),
        name="layer",
    )(*operands)


def local(
    result_cotangent_values,
    specialist_entry_vectors,
    chosen_specialists,
    specialist_mixing_shares,
    specialist_switch_maps,
    specialist_widen_maps,
    specialist_shrink_maps,
    memory_readout_map,
    memory_source_vectors,
    memory_hidden_values,
    feature_fading_speed,
    extra_log_fading,
    memory_switch_tiles,
    entry_switch_tiles,
):
    tok_rows = result_cotangent_values.shape[0]
    sp_count = lax.axis_size(SP)
    expert_count = sp_count // SLICES
    capacity = min(tok_rows, 4 * tok_rows // expert_count)
    dims = (lax.axis_size("sp_0"), lax.axis_size("sp_1"), lax.axis_size("tp"))
    gate_weight_grad, up_weight_grad, down_grad, out_proj_grad, lru_input_grad = layer(
        dims,
        capacity,
        chosen_specialists.T,
        specialist_mixing_shares.T,
        result_cotangent_values,
        specialist_entry_vectors,
        memory_readout_map,
        memory_source_vectors,
        memory_hidden_values,
        feature_fading_speed[None, :],
        extra_log_fading[None, :],
        memory_switch_tiles,
        entry_switch_tiles,
        specialist_switch_maps[0].T,
        specialist_widen_maps[0].T,
        specialist_shrink_maps[0],
    )
    return (
        gate_weight_grad.T[None],
        up_weight_grad.T[None],
        down_grad[None],
        out_proj_grad,
        lru_input_grad,
    )


def solution(mesh):
    finer = Mesh(mesh.devices.reshape(8, 4, 2, mesh.shape["tp"]), ("sp_0", "sp_1", "sp_2", "tp"))
    in_specs = (
        P(SP, None),
        P(SP, None),
        P(SP, None),
        P(SP, None),
        P(SP, None, "tp"),
        P(SP, None, "tp"),
        P(SP, "tp", None),
        P(SP, "tp"),
        P(SP, "tp"),
        P(SP, "tp"),
        P("tp"),
        P(SP),
        P("tp", None, None),
        P("tp", None, None),
    )
    out_specs = (P(SP, None, "tp"), P(SP, None, "tp"), P(SP, "tp", None), P(SP, "tp"), P(SP, "tp"))
    return jax.shard_map(local, mesh=finer, in_specs=in_specs, out_specs=out_specs, check_vma=False)
```

```python
import functools

import jax
import jax.numpy as jnp
from jax import lax
from jax.experimental import pallas as pl
from jax.experimental.pallas import tpu as pltpu
from jax.sharding import Mesh
from jax.sharding import PartitionSpec as P

SLICES = 2
SP = ("sp_0", "sp_1", "sp_2")
MESH = pl.DeviceIdType.MESH
F32, BF16 = jnp.float32, jnp.bfloat16


def place():
    return tuple(lax.axis_index(n) for n in ("sp_0", "sp_1", "sp_2", "tp"))


def offset_of(k, count):
    odd = lax.rem(k, 2)
    return lax.rem(odd * ((k + 1) // 2) + (1 - odd) * (count - k // 2), count)


def drained(ref, sem):
    pltpu.make_async_copy(ref, ref, sem).wait()


def layer_kernel(
    dims, cap, chosen, share, cot, rows, rmap, xmem, hid, fade, extra, rtile, itile, maps,
    outs, proj_out, lru_out,
    slots, xy, wts, flipped, accs, acts, across_acts, give_rows, own_rows, pair, sums, far, near, back, mine, moe, mixed,
    wide, held, turned, cross, fold, rest, levels, pieces, alphas, betas, weights, small, picked,
    in_sem, out_sem, d_send, d_recv, y_send, y_recv, f_send, f_recv, c_send, c_recv,
    p_send, p_recv, e_send, e_recv, r_send, r_recv, m_send, m_recv, b_send, b_recv, z_send, z_recv,
    s_send, s_recv, h_send, h_recv, t_send, t_recv, a_send, a_recv, g_send, g_recv, q_send, q_recv,
):
    nz, nx, ny = dims
    z, x, c, y = place()
    plane = nz * nx * 2
    index = (z * nx + x) * 2 + c
    me = z * nx + x
    toks, feats = cot.shape
    width = feats // ny
    half = nz * nx * cap
    group = nx * cap
    other = (z, x, 1 - c, y)
    up, down = (z, x, c, lax.rem(y + 1, ny)), (z, x, c, lax.rem(y + 3, ny))
    barrier = pltpu.get_barrier_semaphore()

    def sp_at(i):
        i = lax.rem(index + i, plane)
        return (i // (2 * nx), lax.rem(i // 2, nx), lax.rem(i, 2), y)

    def greet(i, _):
        pl.semaphore_signal(barrier, inc=1, device_id=sp_at(i), device_id_type=MESH)
        return 0

    lax.fori_loop(1, plane, greet, 0)
    for step in (1, 2, 3):
        to = (z, x, c, lax.rem(y + step, ny))
        pl.semaphore_signal(barrier, inc=1, device_id=to, device_id_type=MESH)

    def cols(turn):
        return pl.ds(pl.multiple_of(lax.rem(y + turn, ny) * width, 128), width)

    def remote(src, dst, send, recv, to):
        pltpu.make_async_remote_copy(
            src_ref=src, dst_ref=dst, send_sem=send, recv_sem=recv, device_id=to,
            device_id_type=MESH,
        ).start()

    loads = [pltpu.make_async_copy(maps[m], wts.at[m], in_sem.at[m]) for m in range(3)]
    for load in loads:
        load.start()
    wide[z, x, c] = rmap[...]
    held[x, c] = hid[...]

    def upright(line):
        return jnp.transpose(jnp.broadcast_to(line, (toks, toks)))

    experts = [chosen[k : k + 1, :].astype(F32) for k in range(2)]
    earlier = [
        lax.broadcasted_iota(jnp.int32, (toks, toks), 0)
        < lax.broadcasted_iota(jnp.int32, (toks, toks), 1) + k
        for k in range(2)
    ]
    places = []
    for k in range(2):
        rank = jnp.zeros((1, toks), F32)
        for j in range(2):
            same = (upright(experts[j]) == experts[k]) & earlier[1 if j < k else 0]
            rank = rank + jnp.sum(jnp.where(same, 1.0, 0.0), axis=0, keepdims=True)
        places.append(experts[k] * cap + rank)
    slot = lax.broadcasted_iota(jnp.int32, (half, 2 * toks), 0).astype(F32)
    onehot = jnp.where(slot == jnp.concatenate(places, axis=1), 1.0, 0.0).astype(BF16)
    some = rows[:, cols(0)]
    slots[0] = jnp.dot(
        onehot, jnp.concatenate([some, some], axis=0), preferred_element_type=F32
    ).astype(BF16)
    some = cot[:, cols(0)].astype(F32)
    scaled = [(upright(share[k : k + 1, :])[:, 0:1] * some).astype(BF16) for k in range(2)]
    slots[1] = jnp.dot(
        onehot, jnp.concatenate(scaled, axis=0), preferred_element_type=F32
    ).astype(BF16)
    slot = lax.broadcasted_iota(jnp.int32, (toks, half), 1).astype(F32)
    found = [slot == upright(places[k])[:, 0:1] for k in range(2)]
    picked[...] = jnp.where(found[0] | found[1], 1.0, 0.0).astype(BF16)

    def source(e):
        return slots.at[:, pl.ds(pl.multiple_of(e * cap, cap), cap), :]

    mid, piece = nz // 2, half // 2

    def row_of(side, k):
        return (k // mid) * half + side * piece + (k % mid) * group

    def landing(k):
        return xy.at[:, pl.ds(pl.multiple_of(row_of(c, k) + x * cap, cap), cap), cols(0)]

    here = pl.ds(pl.multiple_of(row_of(c, 0) + x * cap, cap), cap)
    mine_too = pl.ds(pl.multiple_of(me * cap, cap), cap)
    for i in range(2):
        xy[i, here, cols(0)] = slots[i, mine_too, :]
    pl.semaphore_wait(barrier, plane - 1 + 3)

    def push(k):
        def one(dx, _):
            tz, tx = lax.rem(z + offset_of(k, nz), nz), lax.rem(x + dx, nx)
            remote(source(tz * nx + tx), landing(k), d_send, d_recv.at[k], (tz, tx, c, y))
            return 0

        lax.fori_loop(1 if k == 0 else 0, nx, one, 0)

    ahead = 3
    push(0)

    def push_rest():
        for step in range(1, nx):
            to = (z, lax.rem(x + step, nx), c, y)
            remote(rmap, wide.at[z, x, c], b_send.at[step - 1], b_recv.at[step - 1], to)
            remote(hid, held.at[x, c], h_send.at[step - 1], h_recv.at[step - 1], to)

    def hand_over():
        for step in range(1, nx):
            drained(hid, h_recv.at[step - 1])
        remote(held.at[:, c], held.at[:, c], t_send, t_recv, other)

    rounds = nz // 2

    def ring_block(s, side, halved):
        away = nz - s if side == 0 else s
        from_z = lax.rem(z + away, nz)
        if halved:
            return wide.at[from_z, pl.ds(side * (nx // 2), nx // 2), c]
        return wide.at[from_z, :, c]

    def ring_sent(s, side):
        return ring_block(s, side, s == rounds - 1)

    def ring(s):
        if s == 0:
            for step in range(1, nx):
                drained(rmap, b_recv.at[step - 1])
            remote(wide.at[z, :, c], wide.at[z, :, c], s_send, s_recv, other)
        else:
            for side in range(2):
                some = ring_block(s, side, s == rounds)
                drained(some, z_recv.at[side, s - 1])
                remote(some, some, s_send, s_recv, other)
        if s < rounds:
            for side in range(2):
                to = (lax.rem(z + (1 if side == 0 else nz - 1), nz), x, c, y)
                some = ring_sent(s, side)
                remote(some, some, z_send.at[side, s], z_recv.at[side, s], to)

    blocks, span = rtile.shape[0], rtile.shape[1]
    row = lax.broadcasted_iota(jnp.int32, (toks, 128), 0)
    reach = [1 << s for s in range(toks.bit_length() - 1)]

    def gates():
        for b in range(blocks):
            here = pl.ds(b * span, span)
            some = xmem[:, here]
            rec = jax.nn.sigmoid(jnp.dot(some, rtile[b], preferred_element_type=F32))
            inp = jax.nn.sigmoid(jnp.dot(some, itile[b], preferred_element_type=F32))
            speed = -8.0 * fade[:, here]
            log_decay = rec * speed + upright(extra[...])[:, 0:1]
            decay = jnp.exp(log_decay)
            spare = 1.0 - jnp.exp(2.0 * log_decay)
            scale = jnp.sqrt(jnp.maximum(spare, 0.01))
            gated = inp * some.astype(F32)
            slope = jnp.where(spare > 0.01, -decay * decay / scale, 0.0)
            level = hid[:, here].astype(F32) - scale * gated + slope * gated
            pieces[0, :, here] = level * speed * rec * (1.0 - rec)
            pieces[1, :, here] = scale * gated * (1.0 - inp)
            pieces[2, :, here] = scale * inp
            pieces[4, :, here] = decay

    def tell(src, dst, send, recv):
        def one(i, _):
            remote(src, dst.at[index], send, recv, sp_at(i))
            return 0

        lax.fori_loop(1, plane, one, 0)

    def products():
        for i in range(width // 128):
            here = pl.ds(i * 128, 128)
            decay = pieces[4, :, here]
            prod = jnp.where(row < toks - 1, pltpu.roll(decay, toks - 1, 0), 1.0)
            for n, s in enumerate(reach):
                inside = row < toks - s
                levels[n, :, here] = jnp.where(inside, prod, 0.0)
                prod = prod * jnp.where(inside, pltpu.roll(prod, toks - s, 0), 1.0)
            pieces[3, :, here] = prod
            small[0, pl.ds(i, 1), :] = decay[0:1] * prod[0:1]
        betas[index] = small[0]
        tell(small.at[0], betas, a_send.at[0], a_recv.at[0])

    def weigh_all():
        drained(betas.at[pl.ds(0, plane - 1)], a_recv.at[0])

        def weigh(j, run):
            later = j > index
            weights[j] = jnp.where(later, run, 0.0)
            return jnp.where(later, run * betas[j], 1.0)

        lax.fori_loop(0, plane, weigh, jnp.ones((width // 128, 128), F32))

    def block(k, turn):
        return xy.at[:, pl.ds(pl.multiple_of(row_of(c, k), cap), group), cols(turn)]

    def across(k, turn):
        remote(block(k, turn), block(k, turn), c_send, c_recv.at[k // mid, turn], other)

    def along(k, turn, to, send, recv):
        remote(block(k, turn), block(k, turn), send, recv, to)

    turn_dims = (((1,), (1,)), ((), ()))
    units = accs.shape[2]

    def flip(m):
        loads[m].wait()

        def some(i, _):
            here = pl.ds(pl.multiple_of(i * 128, 128), 128)
            flipped[m, here, :] = jnp.transpose(wts[m, :, here])
            return 0

        lax.fori_loop(0, feats // 128, some, 0)

    def forward(part, turns):
        here = pl.ds(part * half, half)
        theirs = pl.ds(pl.multiple_of(part * half + (1 - c) * piece, cap), piece)
        for turn in turns:
            drained(xy.at[:, theirs, cols(turn)], c_recv.at[part, turn])

        def some(m, _):
            got = sum(
                jnp.dot(
                    xy[m // 2, here, cols(turn)],
                    flipped[m, cols(turn), :],
                    preferred_element_type=F32,
                )
                for turn in turns
            )
            if 0 in turns:
                accs[m, here, :] = got
            else:
                accs[m, here, :] += got
            return 0

        lax.fori_loop(0, 3, some, 0)

    def activate(part):
        tile = 16

        def some(i, _):
            here = pl.ds(pl.multiple_of(part * half + i * tile, tile), tile)
            gate, wider, backed = accs[0, here, :], accs[1, here, :], accs[2, here, :]
            sig = jax.nn.sigmoid(gate)
            active = gate * sig
            acts[0, here, :] = (backed * wider * (sig * (1.0 + gate * (1.0 - sig)))).astype(BF16)
            acts[1, here, :] = (backed * active).astype(BF16)
            acts[2, here, :] = (active * wider).astype(BF16)
            return 0

        lax.fori_loop(0, half // tile, some, 0)

    chunk = 2 * group
    chunks = nz // 2

    def step_rows(i):
        at = i * chunk
        lines = [
            pl.ds(pl.multiple_of(row_of(side, 2 * i), chunk), chunk) for side in (1 - c, c)
        ]
        left = [jnp.concatenate([acts[m, n, :] for n in lines], axis=0) for m in range(2)]

        def some(n, _):
            here = pl.ds(pl.multiple_of(n * width, 128), width)
            got = jnp.dot(left[0], wts[0, :, here], preferred_element_type=F32)
            got = got + jnp.dot(left[1], wts[1, :, here], preferred_element_type=F32)
            give_rows[pl.ds(at, chunk), here] = got[:chunk].astype(BF16)
            own_rows[pl.ds(at, chunk), here] = got[chunk:].astype(BF16)
            return 0

        lax.fori_loop(0, ny, some, 0)
        span_of = pl.ds(at, chunk)
        remote(give_rows.at[span_of], pair.at[span_of], p_send.at[i], p_recv.at[i], other)

    def step_pair(i):
        at = i * chunk
        span_of = pl.ds(at, chunk)
        drained(pair.at[span_of], p_recv.at[i])
        for turn in (2, 1, 3, 0):
            total = own_rows[span_of, cols(turn)].astype(F32)
            total = total + pair[span_of, cols(turn)].astype(F32)
            sums[turn, span_of, :] = total.astype(BF16)
        low, high = pl.ds(at, group), pl.ds(at + group, group)
        remote(sums.at[2, low], far.at[0, i], e_send.at[0, i], e_recv.at[0, i], up)
        remote(sums.at[2, high], far.at[1, i], e_send.at[1, i], e_recv.at[1, i], down)
        remote(sums.at[1, high], near.at[0, high], e_send.at[2, i], e_recv.at[2, i], up)
        remote(sums.at[3, low], near.at[1, low], e_send.at[3, i], e_recv.at[3, i], down)

    def step_far(i):
        at = i * chunk
        low, high = pl.ds(at, group), pl.ds(at + group, group)
        for side, turn, where, to in ((0, 1, low, up), (1, 3, high, down)):
            drained(far.at[side, i], e_recv.at[side, i])
            total = sums[turn, where, :].astype(F32) + far[side, i].astype(F32)
            sums[turn, where, :] = total.astype(BF16)
            remote(
                sums.at[turn, where], near.at[side, where], e_send.at[4 + side, i],
                e_recv.at[4 + side, i], to,
            )

    def give(i, _):
        k, sx = i // nx, lax.rem(x + lax.rem(i, nx), nx)
        to = (lax.rem(z + nz - offset_of(k, nz), nz), sx, c, y)
        remote(
            mine.at[pl.ds(pl.multiple_of((k * nx + sx) * cap, cap), cap), :],
            back.at[mine_too, :],
            r_send, r_recv, to,
        )
        return 0

    def step_near(i):
        at = i * chunk
        span_of = pl.ds(at, chunk)
        for n in range(2, 6):
            drained(far.at[0, i], e_recv.at[n, i])
        total = sums[0, span_of, :].astype(F32) + near[0, span_of, :].astype(F32)
        mine[span_of, :] = (total + near[1, span_of, :].astype(F32)).astype(BF16)
        k = i * 2
        if k == 0:
            back[mine_too, :] = mine[pl.ds(pl.multiple_of(x * cap, cap), cap), :]
        lax.fori_loop(max(k * nx, 1), (k + 2) * nx, give, 0)

    tall = 256

    def weight_grad(m):
        def turn_over(i, _):
            here = pl.ds(pl.multiple_of(i * 128, 128), 128)
            across_acts[:, here] = jnp.transpose(acts[m, here, :])
            return 0

        lax.fori_loop(0, 2 * half // 128, turn_over, 0)

        def some(i, _):
            here = pl.ds(pl.multiple_of(i * tall, tall), tall)
            wts[m, :, here] = jnp.dot(
                across_acts[...], xy[m // 2, :, here], preferred_element_type=F32
            ).astype(BF16)
            return 0

        lax.fori_loop(0, feats // tall, some, 0)
        pltpu.make_async_copy(wts.at[m], outs[m], out_sem.at[m]).start()

    def receive(k):
        if k == 0:
            drained(slots.at[:, pl.ds(0, group - cap), :], d_recv.at[0])
        else:
            drained(block(k, 0), d_recv.at[k])
        along(k, 0, up, y_send.at[0, k], y_recv.at[0, k])
        along(k, 0, down, y_send.at[1, k], y_recv.at[1, k])
        across(k, 0)
        if k + ahead < nz:
            push(k + ahead)

    def receive_near(k):
        drained(block(k, 3), y_recv.at[0, k])
        if k % 2 == 0:
            along(k, 3, up, f_send.at[k], f_recv.at[k])
        across(k, 3)
        drained(block(k, 1), y_recv.at[1, k])
        if k % 2 == 1:
            along(k, 1, down, f_send.at[k], f_recv.at[k])
        across(k, 1)

    def receive_far(k):
        drained(block(k, 2), f_recv.at[k])
        across(k, 2)

    def work(what, *args):
        return functools.partial(what, *args)

    fillers = {}
    for at, jobs in (
        (0, [work(flip, 2)]),
        (1, [work(flip, 1)]),
        (2, [work(gates), work(products)]),
        (3, [work(push_rest)]),
        (mid + 1, [work(forward, 0, (0,))]),
        (mid + 3, [work(forward, 0, (1, 3))]),
        (nz, [work(forward, 0, (2,)), work(ring, 0)]),
        (nz + 1, [work(activate, 0), work(step_rows, 0), work(forward, 1, (0,))]),
        (nz + 2, [work(step_rows, 1), work(hand_over), work(ring, 1)]),
    ):
        fillers.setdefault(at, []).extend(jobs)
    flip(0)
    for k in range(1, ahead):
        push(k)
    for turn in range(nz + 3):
        if turn < nz:
            receive(turn)
        if 0 <= turn - 2 < nz:
            receive_near(turn - 2)
        if 0 <= turn - 3 < nz - 1:
            receive_far(turn - 3)
        for job in fillers.get(turn, []):
            job()
    early = chunks // 2
    for i in range(early):
        step_pair(i)
    forward(1, (1, 3))
    receive_far(nz - 1)
    forward(1, (2,))
    activate(1)
    for i in range(early):
        step_rows(early + i)
        step_far(i)
    for i in range(early):
        step_pair(early + i)
        step_near(i)
    ring(2)
    for i in range(early):
        step_far(early + i)
    for i in range(early):
        step_near(early + i)
    weight_grad(0)
    weigh_all()
    if rounds > 2:
        ring(3)

    drained(back.at[pl.ds(0, half - cap), :], r_recv)
    moe[:, cols(0)] = jnp.dot(picked[...], back[...], preferred_element_type=F32).astype(BF16)
    for step in (1, 3, 2):
        remote(
            moe.at[:, cols(0)], moe.at[:, cols(0)], m_send.at[step - 1], m_recv.at[step - 1],
            (z, x, c, lax.rem(y + step, ny)),
        )
    weight_grad(1)
    for s in range(4, rounds + 1):
        ring(s)
    drained(wide.at[:, :, 1 - c], s_recv)
    drained(held.at[:, 1 - c], t_recv)
    for step in (1, 3, 2):
        drained(moe.at[:, cols(ny - step)], m_recv.at[step - 1])
    mixed[...] = (cot[...].astype(F32) + moe[...].astype(F32)).astype(BF16)

    lines = rmap.shape[0]
    across_mixed = jnp.transpose(mixed[...]).reshape(nz, 2 * nx, lines, toks)
    for i in range(nz):
        turned[i % 2, i // 2] = across_mixed[i]
    spot = x * 2 + c
    ours = pl.ds(pl.multiple_of(spot * toks, toks), toks)
    cross[:, :, :, ours] = turned[:, :, spot]
    for odd in range(2):
        for step in range(1, 2 * nx):
            to = lax.rem(spot + step, 2 * nx)
            remote(
                turned.at[odd, :, to], cross.at[odd, :, :, ours], g_send.at[odd, step - 1],
                g_recv.at[odd, step - 1], (z, to // 2, lax.rem(to, 2), y),
            )

    state = jnp.dot(mixed[...], wide[...].reshape(-1, width), preferred_element_type=F32)
    for n, s in enumerate(reach):
        state = state + levels[n] * pltpu.roll(state, toks - s, 0)
    first = pieces[4, 0:1, :] * state[0:1]
    for i in range(width // 128):
        small[1, pl.ds(i, 1), :] = first[:, i * 128 : (i + 1) * 128]
    alphas[index] = small[1]
    tell(small.at[1], alphas, a_send.at[1], a_recv.at[1])

    def fold_in(odd):
        for step in range(1, 2 * nx):
            drained(turned.at[0, :, 0], g_recv.at[odd, step - 1])
        total = jnp.dot(
            cross[odd].reshape(mid * lines, 2 * nx * toks),
            held[...].reshape(2 * nx * toks, width),
            preferred_element_type=F32,
        )
        total = total.astype(BF16).reshape(mid, lines, width)
        for i in range(mid):
            fold[2 * i + odd] = total[i]
        for step in range(1, nz):
            to = lax.rem(z + step, nz)

            @pl.when(lax.rem(to, 2) == odd)
            def _():
                remote(
                    fold.at[to], rest.at[z], q_send.at[step - 1], q_recv.at[step - 1], (to, x, c, y)
                )

    fold_in(0)
    fold_in(1)
    rest[z] = fold[z]

    drained(alphas.at[pl.ds(0, plane - 1)], a_recv.at[1])
    carried = jnp.sum(weights[...] * alphas[...], axis=0)
    carried = jnp.concatenate([carried[i : i + 1] for i in range(width // 128)], axis=1)
    state = state + pieces[3] * carried
    grad_rec = (state * pieces[0]).astype(BF16)
    grad_in = (state * pieces[1]).astype(BF16)
    direct = state * pieces[2]
    for b in range(blocks):
        here = slice(b * span, (b + 1) * span)
        lru_out[:, here] = (
            direct[:, here]
            + lax.dot_general(grad_rec[:, here], rtile[b], turn_dims, preferred_element_type=F32)
            + lax.dot_general(grad_in[:, here], itile[b], turn_dims, preferred_element_type=F32)
        )

    weight_grad(2)
    for step in range(1, nz):
        drained(fold.at[0], q_recv.at[step - 1])
    summed = rest[0].astype(F32)
    for i in range(1, nz):
        summed = summed + rest[i].astype(F32)
    proj_out[...] = summed

    drained(xy.at[:, pl.ds(0, half), :], c_send)
    drained(slots.at[:, pl.ds(0, half - cap), :], d_send)
    for k in range(nz):
        drained(block(k, 0), y_send.at[0, k])
        drained(block(k, 0), y_send.at[1, k])
        drained(block(k, 2), f_send.at[k])
    for i in range(chunks):
        drained(pair.at[pl.ds(0, chunk)], p_send.at[i])
        for n in range(6):
            drained(far.at[0, 0], e_send.at[n, i])
    drained(back.at[pl.ds(0, half - cap), :], r_send)
    for step in (1, 2, 3):
        drained(moe.at[:, cols(0)], m_send.at[step - 1])
    for step in range(nx - 1):
        drained(rmap, b_send.at[step])
        drained(hid, h_send.at[step])
    for s in range(rounds):
        for side in range(2):
            drained(ring_sent(s, side), z_send.at[side, s])
    drained(wide.at[:, :, c], s_send)
    drained(held.at[:, c], t_send)
    for i in range(2):
        drained(betas.at[pl.ds(0, plane - 1)], a_send.at[i])
    for step in range(2 * nx - 1):
        for odd in range(2):
            drained(turned.at[0, :, 0], g_send.at[odd, step])
    for step in range(nz - 1):
        drained(fold.at[0], q_send.at[step])
    for m in range(3):
        pltpu.make_async_copy(wts.at[m], outs[m], out_sem.at[m]).wait()


def layer_entry(dims, cap, *refs):
    layer_kernel(dims, cap, *refs[:11], refs[11:14], refs[14:17], *refs[17:])


def layer(dims, cap, *operands):
    chosen, share, cot, rows, rmap, xmem, hid, fade, extra, rtile, itile, *maps = operands
    nz, nx, ny = dims
    toks, feats = cot.shape
    half, width, group = nz * nx * cap, feats // ny, nx * cap
    lines, units = rmap.shape[0], maps[0].shape[0]
    plane, lanes, steps = nz * nx * 2, width // 128, toks.bit_length() - 1
    vmem, anyw = pl.BlockSpec(memory_space=pltpu.VMEM), pl.BlockSpec(memory_space=pl.ANY)
    dma = pltpu.SemaphoreType.DMA
    return pl.pallas_call(
        functools.partial(layer_entry, dims, cap),
        out_shape=[jax.ShapeDtypeStruct((units, feats), BF16)] * 3
        + [
            jax.ShapeDtypeStruct((lines, width), F32),
            jax.ShapeDtypeStruct((toks, width), F32),
        ],
        in_specs=[vmem] * 11 + [anyw] * 3,
        out_specs=[anyw] * 3 + [vmem] * 2,
        scratch_shapes=[
            pltpu.VMEM((2, half, width), BF16),
            pltpu.VMEM((2, 2 * half, feats), BF16),
            pltpu.VMEM((3, units, feats), BF16),
            pltpu.VMEM((3, feats, units), BF16),
            pltpu.VMEM((3, 2 * half, units), F32),
            pltpu.VMEM((3, 2 * half, units), BF16),
            pltpu.VMEM((units, 2 * half), BF16),
            pltpu.VMEM((half, feats), BF16),
            pltpu.VMEM((half, feats), BF16),
            pltpu.VMEM((half, feats), BF16),
            pltpu.VMEM((4, half, width), BF16),
            pltpu.VMEM((2, nz // 2, group, width), BF16),
            pltpu.VMEM((2, half, width), BF16),
            pltpu.VMEM((half, width), BF16),
            pltpu.VMEM((half, width), BF16),
            pltpu.VMEM((toks, feats), BF16),
            pltpu.VMEM((toks, feats), BF16),
            pltpu.VMEM((nz, nx, 2, lines, width), BF16),
            pltpu.VMEM((nx, 2, toks, width), BF16),
            pltpu.VMEM((2, nz // 2, 2 * nx, lines, toks), BF16),
            pltpu.VMEM((2, nz // 2, lines, 2 * nx * toks), BF16),
            pltpu.VMEM((nz, lines, width), BF16),
            pltpu.VMEM((nz, lines, width), BF16),
            pltpu.VMEM((steps, toks, width), F32),
            pltpu.VMEM((5, toks, width), F32),
            pltpu.VMEM((plane, lanes, 128), F32),
            pltpu.VMEM((plane, lanes, 128), F32),
            pltpu.VMEM((plane, lanes, 128), F32),
            pltpu.VMEM((2, lanes, 128), F32),
            pltpu.VMEM((toks, half), BF16),
            dma((3,)), dma((3,)),
            dma, dma((nz,)), dma((2, nz)), dma((2, nz)), dma((nz,)), dma((nz,)), dma, dma((2, 4)),
            dma((nz // 2,)), dma((nz // 2,)), dma((6, nz // 2)), dma((6, nz // 2)), dma, dma,
            dma((3,)), dma((3,)), dma((nx - 1,)), dma((nx - 1,)), dma((2, nz // 2)),
            dma((2, nz // 2)), dma, dma, dma((nx - 1,)), dma((nx - 1,)), dma, dma, dma((2,)),
            dma((2,)), dma((2, 2 * nx - 1)), dma((2, 2 * nx - 1)), dma((nz - 1,)), dma((nz - 1,)),
        ],
        compiler_params=pltpu.CompilerParams(
            collective_id=0, has_side_effects=True, vmem_limit_bytes=60 * 2**20
        ),
        name="layer",
    )(*operands)


def settle_kernel(arrays, parts, *refs):
    ins, outs, held = refs[:arrays], refs[arrays : 2 * arrays], refs[2 * arrays : 3 * arrays]
    in_sem, out_sem = refs[3 * arrays :]
    jobs, n = [], 0
    for i in range(arrays):
        for part in range(parts[i]):
            tall = ins[i].shape[0] // parts[i]
            some = pl.ds(part * tall, tall)
            jobs.append(
                (
                    pltpu.make_async_copy(ins[i].at[some], held[i].at[some], in_sem.at[n]),
                    pltpu.make_async_copy(held[i].at[some], outs[i].at[some], out_sem.at[n]),
                )
            )
            n += 1
    for first, _ in jobs:
        first.start()
    for first, second in jobs:
        first.wait()
        second.start()
    for _, second in jobs:
        second.wait()


def settled(arrays):
    parts = [4 if a.dtype == BF16 else 1 for a in arrays]
    anyw, dma = pl.BlockSpec(memory_space=pl.ANY), pltpu.SemaphoreType.DMA
    return pl.pallas_call(
        functools.partial(settle_kernel, len(arrays), parts),
        out_shape=[jax.ShapeDtypeStruct(a.shape, a.dtype) for a in arrays],
        in_specs=[anyw] * len(arrays),
        out_specs=[anyw] * len(arrays),
        scratch_shapes=[pltpu.VMEM(a.shape, a.dtype) for a in arrays]
        + [dma((sum(parts),)), dma((sum(parts),))],
        compiler_params=pltpu.CompilerParams(vmem_limit_bytes=60 * 2**20),
        name="settle",
    )(*arrays)


def local(
    result_cotangent_values,
    specialist_entry_vectors,
    chosen_specialists,
    specialist_mixing_shares,
    specialist_switch_maps,
    specialist_widen_maps,
    specialist_shrink_maps,
    memory_readout_map,
    memory_source_vectors,
    memory_hidden_values,
    feature_fading_speed,
    extra_log_fading,
    memory_switch_tiles,
    entry_switch_tiles,
):
    tok_rows = result_cotangent_values.shape[0]
    sp_count = lax.axis_size(SP)
    expert_count = sp_count // SLICES
    capacity = min(tok_rows, 4 * tok_rows // expert_count)
    dims = (lax.axis_size("sp_0"), lax.axis_size("sp_1"), lax.axis_size("tp"))
    gate_weight_grad, up_weight_grad, down_grad, out_proj_grad, lru_input_grad = settled(layer(
        dims,
        capacity,
        chosen_specialists.T,
        specialist_mixing_shares.T,
        result_cotangent_values,
        specialist_entry_vectors,
        memory_readout_map,
        memory_source_vectors,
        memory_hidden_values,
        feature_fading_speed[None, :],
        extra_log_fading[None, :],
        memory_switch_tiles,
        entry_switch_tiles,
        specialist_switch_maps[0].T,
        specialist_widen_maps[0].T,
        specialist_shrink_maps[0],
    ))
    return (
        gate_weight_grad.T[None],
        up_weight_grad.T[None],
        down_grad[None],
        out_proj_grad,
        lru_input_grad,
    )


def solution(mesh):
    finer = Mesh(mesh.devices.reshape(8, 4, 2, mesh.shape["tp"]), ("sp_0", "sp_1", "sp_2", "tp"))
    in_specs = (
        P(SP, None),
        P(SP, None),
        P(SP, None),
        P(SP, None),
        P(SP, None, "tp"),
        P(SP, None, "tp"),
        P(SP, "tp", None),
        P(SP, "tp"),
        P(SP, "tp"),
        P(SP, "tp"),
        P("tp"),
        P(SP),
        P("tp", None, None),
        P("tp", None, None),
    )
    out_specs = (P(SP, None, "tp"), P(SP, None, "tp"), P(SP, "tp", None), P(SP, "tp"), P(SP, "tp"))
    return jax.shard_map(local, mesh=finer, in_specs=in_specs, out_specs=out_specs, check_vma=False)
```

```python
import functools

import jax
import jax.numpy as jnp
from jax import lax
from jax.experimental import pallas as pl
from jax.experimental.pallas import tpu as pltpu
from jax.sharding import Mesh
from jax.sharding import PartitionSpec as P

SLICES = 2
SP = ("sp_0", "sp_1", "sp_2")
MESH = pl.DeviceIdType.MESH
F32, BF16 = jnp.float32, jnp.bfloat16


def place():
    return tuple(lax.axis_index(n) for n in ("sp_0", "sp_1", "sp_2", "tp"))


def offset_of(k, count):
    odd = lax.rem(k, 2)
    return lax.rem(odd * ((k + 1) // 2) + (1 - odd) * (count - k // 2), count)


def drained(ref, sem):
    pltpu.make_async_copy(ref, ref, sem).wait()


def layer_kernel(
    dims, cap, chosen, share, cot, rows, rmap, xmem, hid, fade, extra, rtile, itile, maps,
    outs, proj_out, lru_out,
    slots, xy, wts, flipped, accs, acts, across_acts, give_rows, own_rows, pair, sums, far, near, back, mine, moe, mixed,
    wide, held, turned, cross, fold, rest, levels, pieces, alphas, betas, weights, small, picked,
    in_sem, out_sem, d_send, d_recv, y_send, y_recv, f_send, f_recv, c_send, c_recv,
    p_send, p_recv, e_send, e_recv, r_send, r_recv, m_send, m_recv, b_send, b_recv, z_send, z_recv,
    s_send, s_recv, h_send, h_recv, t_send, t_recv, a_send, a_recv, g_send, g_recv, q_send, q_recv,
):
    nz, nx, ny = dims
    z, x, c, y = place()
    plane = nz * nx * 2
    index = (z * nx + x) * 2 + c
    me = z * nx + x
    toks, feats = cot.shape
    width = feats // ny
    half = nz * nx * cap
    group = nx * cap
    other = (z, x, 1 - c, y)
    up, down = (z, x, c, lax.rem(y + 1, ny)), (z, x, c, lax.rem(y + 3, ny))
    barrier = pltpu.get_barrier_semaphore()

    def sp_at(i):
        i = lax.rem(index + i, plane)
        return (i // (2 * nx), lax.rem(i // 2, nx), lax.rem(i, 2), y)

    def greet(i, _):
        pl.semaphore_signal(barrier, inc=1, device_id=sp_at(i), device_id_type=MESH)
        return 0

    lax.fori_loop(1, plane, greet, 0)
    for step in (1, 2, 3):
        to = (z, x, c, lax.rem(y + step, ny))
        pl.semaphore_signal(barrier, inc=1, device_id=to, device_id_type=MESH)

    def cols(turn):
        return pl.ds(pl.multiple_of(lax.rem(y + turn, ny) * width, 128), width)

    def remote(src, dst, send, recv, to):
        pltpu.make_async_remote_copy(
            src_ref=src, dst_ref=dst, send_sem=send, recv_sem=recv, device_id=to,
            device_id_type=MESH,
        ).start()

    loads = [pltpu.make_async_copy(maps[m], wts.at[m], in_sem.at[m]) for m in range(3)]
    for load in loads:
        load.start()
    wide[z, x, c] = rmap[...]
    held[x, c] = hid[...]

    def upright(line):
        return jnp.transpose(jnp.broadcast_to(line, (toks, toks)))

    experts = [chosen[k : k + 1, :].astype(F32) for k in range(2)]
    earlier = [
        lax.broadcasted_iota(jnp.int32, (toks, toks), 0)
        < lax.broadcasted_iota(jnp.int32, (toks, toks), 1) + k
        for k in range(2)
    ]
    places = []
    for k in range(2):
        rank = jnp.zeros((1, toks), F32)
        for j in range(2):
            same = (upright(experts[j]) == experts[k]) & earlier[1 if j < k else 0]
            rank = rank + jnp.sum(jnp.where(same, 1.0, 0.0), axis=0, keepdims=True)
        places.append(experts[k] * cap + rank)
    slot = lax.broadcasted_iota(jnp.int32, (half, 2 * toks), 0).astype(F32)
    onehot = jnp.where(slot == jnp.concatenate(places, axis=1), 1.0, 0.0).astype(BF16)
    some = rows[:, cols(0)]
    slots[0] = jnp.dot(
        onehot, jnp.concatenate([some, some], axis=0), preferred_element_type=F32
    ).astype(BF16)
    some = cot[:, cols(0)].astype(F32)
    scaled = [(upright(share[k : k + 1, :])[:, 0:1] * some).astype(BF16) for k in range(2)]
    slots[1] = jnp.dot(
        onehot, jnp.concatenate(scaled, axis=0), preferred_element_type=F32
    ).astype(BF16)
    slot = lax.broadcasted_iota(jnp.int32, (toks, half), 1).astype(F32)
    found = [slot == upright(places[k])[:, 0:1] for k in range(2)]
    picked[...] = jnp.where(found[0] | found[1], 1.0, 0.0).astype(BF16)

    def source(e):
        return slots.at[:, pl.ds(pl.multiple_of(e * cap, cap), cap), :]

    mid, piece = nz // 2, half // 2

    def row_of(side, k):
        return (k // mid) * half + side * piece + (k % mid) * group

    def landing(k):
        return xy.at[:, pl.ds(pl.multiple_of(row_of(c, k) + x * cap, cap), cap), cols(0)]

    here = pl.ds(pl.multiple_of(row_of(c, 0) + x * cap, cap), cap)
    mine_too = pl.ds(pl.multiple_of(me * cap, cap), cap)
    for i in range(2):
        xy[i, here, cols(0)] = slots[i, mine_too, :]
    pl.semaphore_wait(barrier, plane - 1 + 3)

    def push(k):
        def one(dx, _):
            tz, tx = lax.rem(z + offset_of(k, nz), nz), lax.rem(x + dx, nx)
            remote(source(tz * nx + tx), landing(k), d_send, d_recv.at[k], (tz, tx, c, y))
            return 0

        lax.fori_loop(1 if k == 0 else 0, nx, one, 0)

    ahead = 5
    push(0)

    def push_rest():
        for step in range(1, nx):
            to = (z, lax.rem(x + step, nx), c, y)
            remote(rmap, wide.at[z, x, c], b_send.at[step - 1], b_recv.at[step - 1], to)
            remote(hid, held.at[x, c], h_send.at[step - 1], h_recv.at[step - 1], to)

    def hand_over():
        for step in range(1, nx):
            drained(hid, h_recv.at[step - 1])
        remote(held.at[:, c], held.at[:, c], t_send, t_recv, other)

    rounds = nz // 2

    def ring_block(s, side, halved):
        away = nz - s if side == 0 else s
        from_z = lax.rem(z + away, nz)
        if halved:
            return wide.at[from_z, pl.ds(side * (nx // 2), nx // 2), c]
        return wide.at[from_z, :, c]

    def ring_sent(s, side):
        return ring_block(s, side, s == rounds - 1)

    def ring(s):
        if s == 0:
            for step in range(1, nx):
                drained(rmap, b_recv.at[step - 1])
            remote(wide.at[z, :, c], wide.at[z, :, c], s_send, s_recv, other)
        else:
            for side in range(2):
                some = ring_block(s, side, s == rounds)
                drained(some, z_recv.at[side, s - 1])
                remote(some, some, s_send, s_recv, other)
        if s < rounds:
            for side in range(2):
                to = (lax.rem(z + (1 if side == 0 else nz - 1), nz), x, c, y)
                some = ring_sent(s, side)
                remote(some, some, z_send.at[side, s], z_recv.at[side, s], to)

    blocks, span = rtile.shape[0], rtile.shape[1]
    row = lax.broadcasted_iota(jnp.int32, (toks, 128), 0)
    reach = [1 << s for s in range(toks.bit_length() - 1)]

    def gates():
        for b in range(blocks):
            here = pl.ds(b * span, span)
            some = xmem[:, here]
            rec = jax.nn.sigmoid(jnp.dot(some, rtile[b], preferred_element_type=F32))
            inp = jax.nn.sigmoid(jnp.dot(some, itile[b], preferred_element_type=F32))
            speed = -8.0 * fade[:, here]
            log_decay = rec * speed + upright(extra[...])[:, 0:1]
            decay = jnp.exp(log_decay)
            spare = 1.0 - jnp.exp(2.0 * log_decay)
            scale = jnp.sqrt(jnp.maximum(spare, 0.01))
            gated = inp * some.astype(F32)
            slope = jnp.where(spare > 0.01, -decay * decay / scale, 0.0)
            level = hid[:, here].astype(F32) - scale * gated + slope * gated
            pieces[0, :, here] = level * speed * rec * (1.0 - rec)
            pieces[1, :, here] = scale * gated * (1.0 - inp)
            pieces[2, :, here] = scale * inp
            pieces[4, :, here] = decay

    def tell(src, dst, send, recv):
        def one(i, _):
            remote(src, dst.at[index], send, recv, sp_at(i))
            return 0

        lax.fori_loop(1, plane, one, 0)

    def products():
        for i in range(width // 128):
            here = pl.ds(i * 128, 128)
            decay = pieces[4, :, here]
            prod = jnp.where(row < toks - 1, pltpu.roll(decay, toks - 1, 0), 1.0)
            for n, s in enumerate(reach):
                inside = row < toks - s
                levels[n, :, here] = jnp.where(inside, prod, 0.0)
                prod = prod * jnp.where(inside, pltpu.roll(prod, toks - s, 0), 1.0)
            pieces[3, :, here] = prod
            small[0, pl.ds(i, 1), :] = decay[0:1] * prod[0:1]
        betas[index] = small[0]
        tell(small.at[0], betas, a_send.at[0], a_recv.at[0])

    def weigh_all():
        drained(betas.at[pl.ds(0, plane - 1)], a_recv.at[0])

        def weigh(j, run):
            later = j > index
            weights[j] = jnp.where(later, run, 0.0)
            return jnp.where(later, run * betas[j], 1.0)

        lax.fori_loop(0, plane, weigh, jnp.ones((width // 128, 128), F32))

    def block(k, turn):
        return xy.at[:, pl.ds(pl.multiple_of(row_of(c, k), cap), group), cols(turn)]

    def across(k, turn):
        remote(block(k, turn), block(k, turn), c_send, c_recv.at[k // mid, turn], other)

    def along(k, turn, to, send, recv):
        remote(block(k, turn), block(k, turn), send, recv, to)

    turn_dims = (((1,), (1,)), ((), ()))
    units = accs.shape[2]

    def flip(m):
        loads[m].wait()

        def some(i, _):
            here = pl.ds(pl.multiple_of(i * 128, 128), 128)
            flipped[m, here, :] = jnp.transpose(wts[m, :, here])
            return 0

        lax.fori_loop(0, feats // 128, some, 0)

    def forward(part, turns):
        here = pl.ds(part * half, half)
        theirs = pl.ds(pl.multiple_of(part * half + (1 - c) * piece, cap), piece)
        for turn in turns:
            drained(xy.at[:, theirs, cols(turn)], c_recv.at[part, turn])

        def some(m, _):
            got = sum(
                jnp.dot(
                    xy[m // 2, here, cols(turn)],
                    flipped[m, cols(turn), :],
                    preferred_element_type=F32,
                )
                for turn in turns
            )
            if 0 in turns:
                accs[m, here, :] = got
            else:
                accs[m, here, :] += got
            return 0

        lax.fori_loop(0, 3, some, 0)

    def activate(part):
        tile = 16

        def some(i, _):
            here = pl.ds(pl.multiple_of(part * half + i * tile, tile), tile)
            gate, wider, backed = accs[0, here, :], accs[1, here, :], accs[2, here, :]
            sig = jax.nn.sigmoid(gate)
            active = gate * sig
            acts[0, here, :] = (backed * wider * (sig * (1.0 + gate * (1.0 - sig)))).astype(BF16)
            acts[1, here, :] = (backed * active).astype(BF16)
            acts[2, here, :] = (active * wider).astype(BF16)
            return 0

        lax.fori_loop(0, half // tile, some, 0)

    chunk = 2 * group
    chunks = nz // 2

    def step_rows(i):
        at = i * chunk
        lines = [
            pl.ds(pl.multiple_of(row_of(side, 2 * i), chunk), chunk) for side in (1 - c, c)
        ]
        left = [jnp.concatenate([acts[m, n, :] for n in lines], axis=0) for m in range(2)]

        def some(n, _):
            here = pl.ds(pl.multiple_of(n * width, 128), width)
            got = jnp.dot(left[0], wts[0, :, here], preferred_element_type=F32)
            got = got + jnp.dot(left[1], wts[1, :, here], preferred_element_type=F32)
            give_rows[pl.ds(at, chunk), here] = got[:chunk].astype(BF16)
            own_rows[pl.ds(at, chunk), here] = got[chunk:].astype(BF16)
            return 0

        lax.fori_loop(0, ny, some, 0)
        span_of = pl.ds(at, chunk)
        remote(give_rows.at[span_of], pair.at[span_of], p_send.at[i], p_recv.at[i], other)

    def step_pair(i):
        at = i * chunk
        span_of = pl.ds(at, chunk)
        drained(pair.at[span_of], p_recv.at[i])
        for turn in (2, 1, 3, 0):
            total = own_rows[span_of, cols(turn)].astype(F32)
            total = total + pair[span_of, cols(turn)].astype(F32)
            sums[turn, span_of, :] = total.astype(BF16)
        low, high = pl.ds(at, group), pl.ds(at + group, group)
        remote(sums.at[2, low], far.at[0, i], e_send.at[0, i], e_recv.at[0, i], up)
        remote(sums.at[2, high], far.at[1, i], e_send.at[1, i], e_recv.at[1, i], down)
        remote(sums.at[1, high], near.at[0, high], e_send.at[2, i], e_recv.at[2, i], up)
        remote(sums.at[3, low], near.at[1, low], e_send.at[3, i], e_recv.at[3, i], down)

    def step_far(i):
        at = i * chunk
        low, high = pl.ds(at, group), pl.ds(at + group, group)
        for side, turn, where, to in ((0, 1, low, up), (1, 3, high, down)):
            drained(far.at[side, i], e_recv.at[side, i])
            total = sums[turn, where, :].astype(F32) + far[side, i].astype(F32)
            sums[turn, where, :] = total.astype(BF16)
            remote(
                sums.at[turn, where], near.at[side, where], e_send.at[4 + side, i],
                e_recv.at[4 + side, i], to,
            )

    def give(i, _):
        k, sx = i // nx, lax.rem(x + lax.rem(i, nx), nx)
        to = (lax.rem(z + nz - offset_of(k, nz), nz), sx, c, y)
        remote(
            mine.at[pl.ds(pl.multiple_of((k * nx + sx) * cap, cap), cap), :],
            back.at[mine_too, :],
            r_send, r_recv, to,
        )
        return 0

    def step_near(i):
        at = i * chunk
        span_of = pl.ds(at, chunk)
        for n in range(2, 6):
            drained(far.at[0, i], e_recv.at[n, i])
        total = sums[0, span_of, :].astype(F32) + near[0, span_of, :].astype(F32)
        mine[span_of, :] = (total + near[1, span_of, :].astype(F32)).astype(BF16)
        k = i * 2
        if k == 0:
            back[mine_too, :] = mine[pl.ds(pl.multiple_of(x * cap, cap), cap), :]
        lax.fori_loop(max(k * nx, 1), (k + 2) * nx, give, 0)

    tall = 256

    def weight_grad(m):
        def turn_over(i, _):
            here = pl.ds(pl.multiple_of(i * 128, 128), 128)
            across_acts[:, here] = jnp.transpose(acts[m, here, :])
            return 0

        lax.fori_loop(0, 2 * half // 128, turn_over, 0)

        def some(i, _):
            here = pl.ds(pl.multiple_of(i * tall, tall), tall)
            wts[m, :, here] = jnp.dot(
                across_acts[...], xy[m // 2, :, here], preferred_element_type=F32
            ).astype(BF16)
            return 0

        lax.fori_loop(0, feats // tall, some, 0)
        pltpu.make_async_copy(wts.at[m], outs[m], out_sem.at[m]).start()

    def receive(k):
        if k == 0:
            drained(slots.at[:, pl.ds(0, group - cap), :], d_recv.at[0])
        else:
            drained(block(k, 0), d_recv.at[k])
        along(k, 0, up, y_send.at[0, k], y_recv.at[0, k])
        along(k, 0, down, y_send.at[1, k], y_recv.at[1, k])
        across(k, 0)
        if k + ahead < nz:
            push(k + ahead)

    def receive_near(k):
        drained(block(k, 3), y_recv.at[0, k])
        if k % 2 == 0:
            along(k, 3, up, f_send.at[k], f_recv.at[k])
        across(k, 3)
        drained(block(k, 1), y_recv.at[1, k])
        if k % 2 == 1:
            along(k, 1, down, f_send.at[k], f_recv.at[k])
        across(k, 1)

    def receive_far(k):
        drained(block(k, 2), f_recv.at[k])
        across(k, 2)

    def work(what, *args):
        return functools.partial(what, *args)

    fillers = {}
    for at, jobs in (
        (0, [work(flip, 2)]),
        (1, [work(flip, 1)]),
        (2, [work(gates), work(products)]),
        (3, [work(push_rest)]),
        (mid + 1, [work(forward, 0, (0,))]),
        (mid + 3, [work(forward, 0, (1, 3))]),
        (nz, [work(forward, 0, (2,)), work(ring, 0)]),
        (nz + 1, [work(activate, 0), work(step_rows, 0), work(forward, 1, (0,))]),
        (nz + 2, [work(step_rows, 1), work(hand_over), work(ring, 1)]),
    ):
        fillers.setdefault(at, []).extend(jobs)
    flip(0)
    for k in range(1, ahead):
        push(k)
    for turn in range(nz + 3):
        if turn < nz:
            receive(turn)
        if 0 <= turn - 2 < nz:
            receive_near(turn - 2)
        if 0 <= turn - 3 < nz - 1:
            receive_far(turn - 3)
        for job in fillers.get(turn, []):
            job()
    early = chunks // 2
    for i in range(early):
        step_pair(i)
    forward(1, (1, 3))
    receive_far(nz - 1)
    forward(1, (2,))
    activate(1)
    for i in range(early):
        step_rows(early + i)
        step_far(i)
    for i in range(early):
        step_pair(early + i)
        step_near(i)
    ring(2)
    for i in range(early):
        step_far(early + i)
    for i in range(early):
        step_near(early + i)
    weight_grad(0)
    weigh_all()
    if rounds > 2:
        ring(3)

    drained(back.at[pl.ds(0, half - cap), :], r_recv)
    moe[:, cols(0)] = jnp.dot(picked[...], back[...], preferred_element_type=F32).astype(BF16)
    for step in (1, 3, 2):
        remote(
            moe.at[:, cols(0)], moe.at[:, cols(0)], m_send.at[step - 1], m_recv.at[step - 1],
            (z, x, c, lax.rem(y + step, ny)),
        )
    weight_grad(1)
    for s in range(4, rounds + 1):
        ring(s)
    drained(wide.at[:, :, 1 - c], s_recv)
    drained(held.at[:, 1 - c], t_recv)
    for step in (1, 3, 2):
        drained(moe.at[:, cols(ny - step)], m_recv.at[step - 1])
    mixed[...] = (cot[...].astype(F32) + moe[...].astype(F32)).astype(BF16)

    lines = rmap.shape[0]
    across_mixed = jnp.transpose(mixed[...]).reshape(nz, 2 * nx, lines, toks)
    for i in range(nz):
        turned[i % 2, i // 2] = across_mixed[i]
    spot = x * 2 + c
    ours = pl.ds(pl.multiple_of(spot * toks, toks), toks)
    cross[:, :, :, ours] = turned[:, :, spot]
    for odd in range(2):
        for step in range(1, 2 * nx):
            to = lax.rem(spot + step, 2 * nx)
            remote(
                turned.at[odd, :, to], cross.at[odd, :, :, ours], g_send.at[odd, step - 1],
                g_recv.at[odd, step - 1], (z, to // 2, lax.rem(to, 2), y),
            )

    state = jnp.dot(mixed[...], wide[...].reshape(-1, width), preferred_element_type=F32)
    for n, s in enumerate(reach):
        state = state + levels[n] * pltpu.roll(state, toks - s, 0)
    first = pieces[4, 0:1, :] * state[0:1]
    for i in range(width // 128):
        small[1, pl.ds(i, 1), :] = first[:, i * 128 : (i + 1) * 128]
    alphas[index] = small[1]
    tell(small.at[1], alphas, a_send.at[1], a_recv.at[1])

    def fold_in(odd):
        for step in range(1, 2 * nx):
            drained(turned.at[0, :, 0], g_recv.at[odd, step - 1])
        total = jnp.dot(
            cross[odd].reshape(mid * lines, 2 * nx * toks),
            held[...].reshape(2 * nx * toks, width),
            preferred_element_type=F32,
        )
        total = total.astype(BF16).reshape(mid, lines, width)
        for i in range(mid):
            fold[2 * i + odd] = total[i]
        for step in range(1, nz):
            to = lax.rem(z + step, nz)

            @pl.when(lax.rem(to, 2) == odd)
            def _():
                remote(
                    fold.at[to], rest.at[z], q_send.at[step - 1], q_recv.at[step - 1], (to, x, c, y)
                )

    fold_in(0)
    fold_in(1)
    rest[z] = fold[z]

    drained(alphas.at[pl.ds(0, plane - 1)], a_recv.at[1])
    carried = jnp.sum(weights[...] * alphas[...], axis=0)
    carried = jnp.concatenate([carried[i : i + 1] for i in range(width // 128)], axis=1)
    state = state + pieces[3] * carried
    grad_rec = (state * pieces[0]).astype(BF16)
    grad_in = (state * pieces[1]).astype(BF16)
    direct = state * pieces[2]
    for b in range(blocks):
        here = slice(b * span, (b + 1) * span)
        lru_out[:, here] = (
            direct[:, here]
            + lax.dot_general(grad_rec[:, here], rtile[b], turn_dims, preferred_element_type=F32)
            + lax.dot_general(grad_in[:, here], itile[b], turn_dims, preferred_element_type=F32)
        )

    weight_grad(2)
    for step in range(1, nz):
        drained(fold.at[0], q_recv.at[step - 1])
    summed = rest[0].astype(F32)
    for i in range(1, nz):
        summed = summed + rest[i].astype(F32)
    proj_out[...] = summed

    drained(xy.at[:, pl.ds(0, half), :], c_send)
    drained(slots.at[:, pl.ds(0, half - cap), :], d_send)
    for k in range(nz):
        drained(block(k, 0), y_send.at[0, k])
        drained(block(k, 0), y_send.at[1, k])
        drained(block(k, 2), f_send.at[k])
    for i in range(chunks):
        drained(pair.at[pl.ds(0, chunk)], p_send.at[i])
        for n in range(6):
            drained(far.at[0, 0], e_send.at[n, i])
    drained(back.at[pl.ds(0, half - cap), :], r_send)
    for step in (1, 2, 3):
        drained(moe.at[:, cols(0)], m_send.at[step - 1])
    for step in range(nx - 1):
        drained(rmap, b_send.at[step])
        drained(hid, h_send.at[step])
    for s in range(rounds):
        for side in range(2):
            drained(ring_sent(s, side), z_send.at[side, s])
    drained(wide.at[:, :, c], s_send)
    drained(held.at[:, c], t_send)
    for i in range(2):
        drained(betas.at[pl.ds(0, plane - 1)], a_send.at[i])
    for step in range(2 * nx - 1):
        for odd in range(2):
            drained(turned.at[0, :, 0], g_send.at[odd, step])
    for step in range(nz - 1):
        drained(fold.at[0], q_send.at[step])
    for m in range(3):
        pltpu.make_async_copy(wts.at[m], outs[m], out_sem.at[m]).wait()


def layer_entry(dims, cap, *refs):
    layer_kernel(dims, cap, *refs[:11], refs[11:14], refs[14:17], *refs[17:])


def layer(dims, cap, *operands):
    chosen, share, cot, rows, rmap, xmem, hid, fade, extra, rtile, itile, *maps = operands
    nz, nx, ny = dims
    toks, feats = cot.shape
    half, width, group = nz * nx * cap, feats // ny, nx * cap
    lines, units = rmap.shape[0], maps[0].shape[0]
    plane, lanes, steps = nz * nx * 2, width // 128, toks.bit_length() - 1
    vmem, anyw = pl.BlockSpec(memory_space=pltpu.VMEM), pl.BlockSpec(memory_space=pl.ANY)
    dma = pltpu.SemaphoreType.DMA
    return pl.pallas_call(
        functools.partial(layer_entry, dims, cap),
        out_shape=[jax.ShapeDtypeStruct((units, feats), BF16)] * 3
        + [
            jax.ShapeDtypeStruct((lines, width), F32),
            jax.ShapeDtypeStruct((toks, width), F32),
        ],
        in_specs=[vmem] * 11 + [anyw] * 3,
        out_specs=[anyw] * 3 + [vmem] * 2,
        scratch_shapes=[
            pltpu.VMEM((2, half, width), BF16),
            pltpu.VMEM((2, 2 * half, feats), BF16),
            pltpu.VMEM((3, units, feats), BF16),
            pltpu.VMEM((3, feats, units), BF16),
            pltpu.VMEM((3, 2 * half, units), F32),
            pltpu.VMEM((3, 2 * half, units), BF16),
            pltpu.VMEM((units, 2 * half), BF16),
            pltpu.VMEM((half, feats), BF16),
            pltpu.VMEM((half, feats), BF16),
            pltpu.VMEM((half, feats), BF16),
            pltpu.VMEM((4, half, width), BF16),
            pltpu.VMEM((2, nz // 2, group, width), BF16),
            pltpu.VMEM((2, half, width), BF16),
            pltpu.VMEM((half, width), BF16),
            pltpu.VMEM((half, width), BF16),
            pltpu.VMEM((toks, feats), BF16),
            pltpu.VMEM((toks, feats), BF16),
            pltpu.VMEM((nz, nx, 2, lines, width), BF16),
            pltpu.VMEM((nx, 2, toks, width), BF16),
            pltpu.VMEM((2, nz // 2, 2 * nx, lines, toks), BF16),
            pltpu.VMEM((2, nz // 2, lines, 2 * nx * toks), BF16),
            pltpu.VMEM((nz, lines, width), BF16),
            pltpu.VMEM((nz, lines, width), BF16),
            pltpu.VMEM((steps, toks, width), F32),
            pltpu.VMEM((5, toks, width), F32),
            pltpu.VMEM((plane, lanes, 128), F32),
            pltpu.VMEM((plane, lanes, 128), F32),
            pltpu.VMEM((plane, lanes, 128), F32),
            pltpu.VMEM((2, lanes, 128), F32),
            pltpu.VMEM((toks, half), BF16),
            dma((3,)), dma((3,)),
            dma, dma((nz,)), dma((2, nz)), dma((2, nz)), dma((nz,)), dma((nz,)), dma, dma((2, 4)),
            dma((nz // 2,)), dma((nz // 2,)), dma((6, nz // 2)), dma((6, nz // 2)), dma, dma,
            dma((3,)), dma((3,)), dma((nx - 1,)), dma((nx - 1,)), dma((2, nz // 2)),
            dma((2, nz // 2)), dma, dma, dma((nx - 1,)), dma((nx - 1,)), dma, dma, dma((2,)),
            dma((2,)), dma((2, 2 * nx - 1)), dma((2, 2 * nx - 1)), dma((nz - 1,)), dma((nz - 1,)),
        ],
        compiler_params=pltpu.CompilerParams(
            collective_id=0, has_side_effects=True, vmem_limit_bytes=60 * 2**20
        ),
        name="layer",
    )(*operands)


def settle_kernel(arrays, parts, *refs):
    ins, outs, held = refs[:arrays], refs[arrays : 2 * arrays], refs[2 * arrays : 3 * arrays]
    in_sem, out_sem = refs[3 * arrays :]
    jobs, n = [], 0
    for i in range(arrays):
        for part in range(parts[i]):
            tall = ins[i].shape[0] // parts[i]
            some = pl.ds(part * tall, tall)
            jobs.append(
                (
                    pltpu.make_async_copy(ins[i].at[some], held[i].at[some], in_sem.at[n]),
                    pltpu.make_async_copy(held[i].at[some], outs[i].at[some], out_sem.at[n]),
                )
            )
            n += 1
    for first, _ in jobs:
        first.start()
    for first, second in jobs:
        first.wait()
        second.start()
    for _, second in jobs:
        second.wait()


def settled(arrays):
    parts = [4 if a.dtype == BF16 else 1 for a in arrays]
    anyw, dma = pl.BlockSpec(memory_space=pl.ANY), pltpu.SemaphoreType.DMA
    return pl.pallas_call(
        functools.partial(settle_kernel, len(arrays), parts),
        out_shape=[jax.ShapeDtypeStruct(a.shape, a.dtype) for a in arrays],
        in_specs=[anyw] * len(arrays),
        out_specs=[anyw] * len(arrays),
        scratch_shapes=[pltpu.VMEM(a.shape, a.dtype) for a in arrays]
        + [dma((sum(parts),)), dma((sum(parts),))],
        compiler_params=pltpu.CompilerParams(vmem_limit_bytes=60 * 2**20),
        name="settle",
    )(*arrays)


def local(
    result_cotangent_values,
    specialist_entry_vectors,
    chosen_specialists,
    specialist_mixing_shares,
    specialist_switch_maps,
    specialist_widen_maps,
    specialist_shrink_maps,
    memory_readout_map,
    memory_source_vectors,
    memory_hidden_values,
    feature_fading_speed,
    extra_log_fading,
    memory_switch_tiles,
    entry_switch_tiles,
):
    tok_rows = result_cotangent_values.shape[0]
    sp_count = lax.axis_size(SP)
    expert_count = sp_count // SLICES
    capacity = min(tok_rows, 4 * tok_rows // expert_count)
    dims = (lax.axis_size("sp_0"), lax.axis_size("sp_1"), lax.axis_size("tp"))
    gate_weight_grad, up_weight_grad, down_grad, out_proj_grad, lru_input_grad = settled(layer(
        dims,
        capacity,
        chosen_specialists.T,
        specialist_mixing_shares.T,
        result_cotangent_values,
        specialist_entry_vectors,
        memory_readout_map,
        memory_source_vectors,
        memory_hidden_values,
        feature_fading_speed[None, :],
        extra_log_fading[None, :],
        memory_switch_tiles,
        entry_switch_tiles,
        specialist_switch_maps[0].T,
        specialist_widen_maps[0].T,
        specialist_shrink_maps[0],
    ))
    return (
        gate_weight_grad.T[None],
        up_weight_grad.T[None],
        down_grad[None],
        out_proj_grad,
        lru_input_grad,
    )


def solution(mesh):
    finer = Mesh(mesh.devices.reshape(8, 4, 2, mesh.shape["tp"]), ("sp_0", "sp_1", "sp_2", "tp"))
    in_specs = (
        P(SP, None),
        P(SP, None),
        P(SP, None),
        P(SP, None),
        P(SP, None, "tp"),
        P(SP, None, "tp"),
        P(SP, "tp", None),
        P(SP, "tp"),
        P(SP, "tp"),
        P(SP, "tp"),
        P("tp"),
        P(SP),
        P("tp", None, None),
        P("tp", None, None),
    )
    out_specs = (P(SP, None, "tp"), P(SP, None, "tp"), P(SP, "tp", None), P(SP, "tp"), P(SP, "tp"))
    return jax.shard_map(local, mesh=finer, in_specs=in_specs, out_specs=out_specs, check_vma=False)
```
